1024 devices in a mesh: ep: 32 (over z, core), tp: 32 (over y, x).
Axes of the slice: x: 4, y: 8, z: 16, core: 2. Of those that a mesh axis runs over, the one named last changes fastest.
Arguments:
- tokens: bfloat16 [8192, 4096], P('ep', 'tp'), may hold values from -2000 to 2000, as said below
- norm_gain: float32 [4096], P('tp'), may hold values from 0.1 to 1.9
- route_ids: int32 [8192, 2], P('ep'), may hold values from 0 to 63, all different within a row; in each aligned block of 256 rows (0 to 255, 256 to 511, ...) at most 10 rows name the same one
- route_gates: float32 [8192, 2], P('ep'), may hold values from 0.1 to 1
- w_gate: bfloat16 [64, 768, 4096], P('ep', None, 'tp'), may hold values from -0.09375 to 0.09375
- w_up: bfloat16 [64, 768, 4096], P('ep', None, 'tp'), may hold values from -0.09375 to 0.09375
- w_down: bfloat16 [64, 768, 4096], P('ep', None, 'tp'), may hold values from -0.21875 to 0.21875
Outputs:
- mixed: bfloat16 [8192, 4096], P('ep', 'tp')
The draws below stay inside these ranges and needn't reach their ends.
Inputs may be any that keep to these rules, and one draw needn't show every extreme that they name: `route_ids`: each row names 2 different experts; among the 256 rows of one index of ep no expert is named by more than 10 rows, a bound that some block reaches. `tokens`: finite values.
All inputs are finite; a program needn't handle non-finite values.
Results may differ from the reference program's by a relative error of at most 0.025.
Values may be sent and summed in bfloat16 or wider, within the bound.
A program may use at most 32 MiB of HBM per device.

```python
import math
import jax
import jax.numpy as jnp
import numpy as np
from jax import lax

D = 4096
FF = 768
TOK_EP = 256
TOP_K = 2
EXPERTS = 64
TOKENS = 8192
CAP = 10
N_EP = 32
N_TP = 32


def draw_tokens(key, part):
    first, second, third = jax.random.split(jax.random.fold_in(key, 11), 3)
    columns = jnp.arange(D, dtype=jnp.float32)
    col_scale = 3.0 ** (columns / D) * jnp.exp(jax.random.uniform(second, (D,), jnp.float32) * math.log(4.0))
    row_scale = jnp.exp(jax.random.uniform(third, (TOKENS, 1), jnp.float32) * math.log(10.0))
    base = jax.random.normal(first, (TOKENS, D), jnp.float32)
    return (base * row_scale * col_scale[None, :]).astype(jnp.bfloat16)


def levels(rng, shape, cuts, low, largest):
    level, own = 1.0, jax.random.fold_in(rng, 6)
    for position, shards_of in cuts:
        steps = jnp.exp(jax.random.uniform(jax.random.fold_in(own, position), (shards_of,), jnp.float32, low / len(cuts), largest / len(cuts)))
        level = level * jnp.repeat(steps, shape[position] // shards_of).reshape([-1 if axis == position else 1 for axis in range(len(shape))])
    return level


def shared_out(key, own, number, rows, count, top, most, lean):
    ranking = jax.random.permutation(key, count)
    heavy_load, common = portions_of(count, rows * top, most, lean, True), portions_of(count, rows * top, most, lean, False)
    places = jnp.arange(count)

    def named(tallies, turn):
        used = int((tallies > 0).sum())
        fixed = max(1, used // 4)
        moved = fixed + (places - fixed + turn * (used - fixed)) % max(1, count - fixed)
        return jnp.zeros((count,), jnp.int32).at[ranking[jnp.where(places < fixed, places, moved)]].set(jnp.asarray(tallies, jnp.int32))

    tallies = jnp.where(number % 4 == 0, named(heavy_load, number // 4), named(common, number - number // 4 - 1))
    mixed = jax.random.permutation(jax.random.fold_in(own, 3), count)
    donor, receiver = mixed[0:count // 2 * 2:2], mixed[1:count // 2 * 2:2]
    margin = jnp.minimum(tallies[donor] - 1, most - tallies[receiver]) // 2
    margin = jnp.where((donor == ranking[0]) | (receiver == ranking[0]) | (tallies[receiver] == 0), 0, jnp.maximum(margin, 0))
    moved = jax.random.randint(jax.random.fold_in(own, 4), (count // 2,), 0, 1 << 20) % (margin + 1)
    tallies = tallies.at[donor].add(-moved).at[receiver].add(moved)
    items = jnp.searchsorted(jnp.cumsum(tallies), jnp.arange(rows * top), side="right").astype(jnp.int32)
    grid = items.reshape(top, rows).T
    grid = grid[jax.random.permutation(jax.random.fold_in(own, 1), rows)]
    turn = jax.random.randint(jax.random.fold_in(own, 2), (rows, 1), 0, top)
    return jnp.take_along_axis(grid, (jnp.arange(top)[None, :] + turn) % top, axis=1)


def portions_of(amount, total, reach, skew, full):
    portions = [(1 << 20) // math.isqrt(standing ** skew) + 1 for standing in range(1, amount + 1)]
    largest = reach if full else min(reach, max(-(-total // amount), total * portions[0] // sum(portions)))
    least = 1 if total - largest >= amount - 1 else 0
    holding, surplus = [largest] + [least] * (amount - 1), total - largest - least * (amount - 1)
    while surplus > 0:
        free = [i for i in range(1, amount) if holding[i] < largest] or [i for i in range(1, amount) if holding[i] < reach]
        whole, left = sum([portions[i] for i in free]), surplus
        for i in free:
            addition = min(reach - holding[i], max(1, left * portions[i] // whole), surplus)
            holding[i] = holding[i] + addition
            surplus = surplus - addition
    return np.array(holding)


def normal_values(own_key, extent, spread, reach, cuts=(), held_as=jnp.bfloat16):
    entries = spread * jax.random.normal(own_key, extent, jnp.float32)
    if cuts:
        entries = entries * levels(own_key, extent, cuts, -0.22, 0.18)
    return jnp.clip(entries, -reach, reach).astype(held_as)


def setup_inputs(seed: int = 0) -> dict:
    seeds = jax.random.split(jax.random.key(seed), 8)
    tokens = draw_tokens(jax.random.fold_in(seeds[7], 71), 0)
    norm_gain = jnp.clip(1.0 + 0.18 * jax.random.normal(seeds[1], (D,), jnp.float32), 0.1, 1.9)
    route_ids_keys = jax.random.split(jax.random.fold_in(seeds[2], 1), TOKENS // TOK_EP)
    route_ids_turns = jax.random.permutation(jax.random.fold_in(seeds[2], 3), TOKENS // TOK_EP)
    route_ids = jax.vmap(lambda own, number: shared_out(jax.random.fold_in(seeds[2], 2), own, number, TOK_EP, EXPERTS, TOP_K, CAP, 2))(route_ids_keys, route_ids_turns).reshape((TOKENS, TOP_K))
    route_gates = jnp.clip(0.1 + 0.9 * jax.random.uniform(seeds[3], (TOKENS, TOP_K), jnp.float32) ** levels(seeds[3], (TOKENS, TOP_K), ((0, 32),), -0.2, 0.2), 0.1, 1.0)
    w_gate = normal_values(seeds[4], (EXPERTS, FF, D), D ** -0.5, 0.09375, ((0, 32), (2, 32)))
    w_up = normal_values(seeds[5], (EXPERTS, FF, D), D ** -0.5, 0.09375, ((0, 32), (2, 32)))
    w_down = normal_values(seeds[6], (EXPERTS, FF, D), FF ** -0.5, 0.21875, ((0, 32), (2, 32)))
    return {"tokens": tokens, "norm_gain": norm_gain, "route_ids": route_ids, "route_gates": route_gates, "w_gate": w_gate, "w_up": w_up, "w_down": w_down}


EPSILON = 1e-06

def split_product(rows, weight):
    width = rows.shape[1] // N_TP
    blocks = rows.astype(jnp.float32).reshape(rows.shape[0], N_TP, width)
    wblocks = weight.astype(jnp.float32).reshape(weight.shape[0], N_TP, width)
    partial_value = jnp.einsum('rnc,fnc->nrf', blocks, wblocks)
    return lax.optimization_barrier(jnp.sum(partial_value.astype(jnp.bfloat16).astype(jnp.float32), axis=0))

def reference(tokens, norm_gain, route_ids, route_gates, w_gate, w_up, w_down):
    values = tokens.astype(jnp.float32)
    inverse = lax.rsqrt(lax.optimization_barrier(jnp.mean(values * values, axis=1, keepdims=True)) + EPSILON)
    normed = (values * inverse * norm_gain[None, :]).astype(jnp.bfloat16)
    total_tok = tokens.shape[0]
    flat_ids = route_ids.reshape(N_EP, TOK_EP * TOP_K).astype(jnp.int32)
    onehot = (flat_ids[:, :, None] == jnp.arange(EXPERTS, dtype=jnp.int32)[None, None, :]).astype(jnp.int32)
    before = jnp.cumsum(onehot, axis=1) - onehot
    slot_of = lax.optimization_barrier(jnp.sum(before * onehot, axis=2))
    source = jnp.arange(N_EP, dtype=jnp.int32)[:, None]
    target = ((flat_ids * N_EP + source) * CAP + slot_of).reshape(-1).astype(jnp.int32)
    owners = jnp.repeat(jnp.arange(total_tok, dtype=jnp.int32), TOP_K)
    table = jnp.full((EXPERTS * N_EP * CAP,), total_tok, jnp.int32).at[target].set(owners)
    padded = jnp.concatenate([normed, jnp.zeros((1, D), jnp.bfloat16)], axis=0)

    def run_expert(inputs):
        index_rows, gate_w, up_w, down_w = inputs
        gathered = padded[index_rows]
        gate_act = split_product(gathered, gate_w)
        up_act = split_product(gathered, up_w)
        hidden = (jax.nn.silu(gate_act) * up_act).astype(jnp.bfloat16)
        return jnp.dot(hidden, down_w, preferred_element_type=jnp.float32).astype(jnp.bfloat16)
    outputs = lax.map(run_expert, (table.reshape(EXPERTS, N_EP * CAP), w_gate, w_up, w_down))
    picked = outputs.reshape(EXPERTS * N_EP * CAP, D)[target]
    weighted = picked.astype(jnp.float32).reshape(total_tok, TOP_K, D) * route_gates.astype(jnp.float32)[:, :, None]
    return lax.optimization_barrier(jnp.sum(weighted, axis=1)).astype(jnp.bfloat16)
```

```python
import functools

import jax
import jax.numpy as jnp
from jax import lax
from jax.experimental import pallas as pl
from jax.experimental.pallas import tpu as pltpu
from jax.sharding import PartitionSpec as P

EPSILON = 1e-06
NX = 4
PAD = 16
MESH = pl.DeviceIdType.MESH
F32 = jnp.float32
BF16 = jnp.bfloat16


def dot_nt(a, b):
    return lax.dot_general(a, b, (((1,), (1,)), ((), ())), preferred_element_type=F32)


def dot_nn(a, b):
    return lax.dot_general(a, b, (((1,), (0,)), ((), ())), preferred_element_type=F32)


def kernel(
    n_ep, ny, cap,
    tok_ref, gain_ref, ids_ref, gates_ref, wg_ref, wu_ref, wd_ref,
    out_ref,
    zsend, zrecv, xg, wland, wcat, wdn, gain_all, xs, part, rs, ssq, ssq_all,
    hid, po, xr, back, ret, tcol,
    z_ss, z_rs, r_ss, r_rs, w_ss, w_rs, g_ss, g_rs, x_ss, x_rs,
    y_ss, y_rs, q_ss, q_rs, h_ss, h_rs, o_ss, o_rs, l_sem,
):
    nz = n_ep // 2
    rows = n_ep * PAD
    own = n_ep // ny
    toks = tok_ref.shape[0]
    experts = 2 * n_ep
    half = wg_ref.shape[1] // 2
    feats = tok_ref.shape[1]
    ep = lax.axis_index("ep")
    tp = lax.axis_index("tp")
    z, core = ep // 2, lax.rem(ep, 2)
    y, x = tp // NX, lax.rem(tp, NX)

    def z_peer(i):
        j, c = i // 2, lax.rem(i, 2)
        dz = nz // 2 + (1 - 2 * lax.rem(j, 2)) * ((j + 1) // 2)
        return 2 * lax.rem(z + dz, nz) + c

    def x_peer(k):
        return lax.rem(x + k, NX)

    def y_peer(k):
        return lax.rem(y + k, ny)

    partner = z * 2 + (1 - core)
    x_steps = (2, 1, 3)
    y_steps = sorted(range(1, ny), key=lambda k: -min(k, ny - k))

    barrier = pltpu.get_barrier_semaphore()

    def greet(i, carry):
        pl.semaphore_signal(barrier, inc=1, device_id=(z_peer(i), tp), device_id_type=MESH)
        return carry

    lax.fori_loop(0, 2 * (nz - 1), greet, 0)
    pl.semaphore_signal(barrier, inc=1, device_id=(partner, tp), device_id_type=MESH)
    for k in x_steps:
        pl.semaphore_signal(barrier, inc=1, device_id=(ep, y * NX + x_peer(k)), device_id_type=MESH)
    for k in y_steps:
        pl.semaphore_signal(barrier, inc=1, device_id=(ep, y_peer(k) * NX + x), device_id_type=MESH)

    def w_src(ref, to):
        return ref.at[to // 2, pl.ds(lax.rem(to, 2) * half, half), :]

    own_w = [
        pltpu.make_async_copy(w_src(ref, x), wland.at[n, x], l_sem.at[n])
        for n, ref in enumerate((wg_ref, wu_ref, wd_ref))
    ]
    for copy in own_w:
        copy.start()

    ids = ids_ref[...].astype(F32)
    e_iota = lax.broadcasted_iota(jnp.int32, (experts, toks), 0).astype(F32)
    m0, m1 = e_iota == ids[0:1, :], e_iota == ids[1:2, :]
    named = jnp.where(m0 | m1, 1.0, 0.0).astype(BF16)
    t_row = lax.broadcasted_iota(jnp.int32, (toks, toks), 0)
    t_col = lax.broadcasted_iota(jnp.int32, (toks, toks), 1)
    earlier = jnp.where(t_row < t_col, 1.0, 0.0).astype(BF16)
    before = dot_nn(named, earlier)
    target0 = ids[0:1, :] * PAD + jnp.sum(jnp.where(m0, before, 0.0), axis=0, keepdims=True)
    target1 = ids[1:2, :] * PAD + jnp.sum(jnp.where(m1, before, 0.0), axis=0, keepdims=True)
    chunk = min(256, experts * PAD)
    for n in range(experts * PAD // chunk):
        p_iota = (lax.broadcasted_iota(jnp.int32, (chunk, toks), 0) + n * chunk).astype(F32)
        pick = jnp.where((p_iota == target0) | (p_iota == target1), 1.0, 0.0).astype(BF16)
        block = dot_nn(pick, tok_ref[...]).astype(BF16)
        zsend[pl.ds(n * chunk // PAD, chunk // PAD)] = block.reshape(chunk // PAD, PAD, feats)
    ret[...] = jnp.zeros_like(ret)
    gain_all[x] = gain_ref[...]

    pl.semaphore_wait(barrier, 2 * nz - 1 + (NX - 1) + (ny - 1))

    def z_copy(peer):
        return pltpu.make_async_remote_copy(
            src_ref=zsend.at[pl.ds(2 * peer, 2), pl.ds(0, cap)],
            dst_ref=zrecv.at[:, ep, pl.ds(0, cap)],
            send_sem=z_ss.at[peer], recv_sem=z_rs.at[ep],
            device_id=(peer, tp), device_id_type=MESH,
        )

    def z_arrival(peer):
        return pltpu.make_async_remote_copy(
            src_ref=zsend.at[pl.ds(2 * peer, 2), pl.ds(0, cap)],
            dst_ref=zrecv.at[:, peer, pl.ds(0, cap)],
            send_sem=z_ss.at[peer], recv_sem=z_rs.at[peer],
            device_id=(peer, tp), device_id_type=MESH,
        )

    def each_z(fn):
        def step(i, carry):
            fn(z_peer(i))
            return carry

        lax.fori_loop(0, 2 * (nz - 1), step, 0)
        fn(partner)

    each_z(lambda peer: z_copy(peer).start())

    def w_copy(n, ref, k, slot):
        return pltpu.make_async_remote_copy(
            src_ref=w_src(ref, x_peer(k)), dst_ref=wland.at[n, slot],
            send_sem=w_ss.at[n, k], recv_sem=w_rs.at[n, k],
            device_id=(ep, y * NX + x_peer(k)), device_id_type=MESH,
        )

    def g_copy(k, slot):
        return pltpu.make_async_remote_copy(
            src_ref=gain_ref, dst_ref=gain_all.at[slot],
            send_sem=g_ss.at[k], recv_sem=g_rs.at[k],
            device_id=(ep, y * NX + x_peer(k)), device_id_type=MESH,
        )

    weights = list(enumerate((wg_ref, wu_ref, wd_ref)))
    for k in x_steps:
        g_copy(k, x).start()
    for n, ref in weights:
        for k in x_steps:
            w_copy(n, ref, k, x).start()

    zrecv[0, ep] = zsend[2 * ep]
    zrecv[1, ep] = zsend[2 * ep + 1]

    pad_rows = jnp.zeros((124, toks), F32)
    tcol[...] = jnp.concatenate([target0, target1, gates_ref[...], pad_rows], axis=0).T

    each_z(lambda peer: z_arrival(peer).wait_recv())

    def x_copy(k, slot):
        to = x_peer(k)
        return pltpu.make_async_remote_copy(
            src_ref=zrecv.at[to // 2, :, pl.ds(0, cap)], dst_ref=xg.at[slot, :, pl.ds(0, cap)],
            send_sem=x_ss.at[k], recv_sem=x_rs.at[k],
            device_id=(ep, y * NX + to), device_id_type=MESH,
        )

    for k in x_steps:
        x_copy(k, x).start()
    xg[x] = zrecv[x // 2]

    def came(k):
        return lax.rem(x + NX - k, NX)

    for copy in own_w:
        copy.wait()
    for k in x_steps:
        g_copy(k, came(k)).wait_recv()
        for n, ref in weights:
            w_copy(n, ref, k, came(k)).wait_recv()
    for s in range(NX):
        wcat[0:half, s * feats : (s + 1) * feats] = wland[0, s]
        wcat[half : 2 * half, s * feats : (s + 1) * feats] = wland[1, s]
        wdn[:, s * feats : (s + 1) * feats] = wland[2, s]

    for k in x_steps:
        x_copy(k, came(k)).wait_recv()

    squares = jnp.zeros((rows, feats), F32)
    for s in range(NX):
        raw = xg[s].reshape(rows, feats).astype(F32)
        squares += raw * raw
        xs[:, s * feats : (s + 1) * feats] = (raw * gain_all[s]).astype(BF16)
    sums = jnp.sum(squares, axis=1, keepdims=True)
    lane = lax.broadcasted_iota(jnp.int32, (rows, 128), 1)
    row = lax.broadcasted_iota(jnp.int32, (rows, 128), 0)
    spread = jnp.where(lane == lax.rem(row, 128), sums, 0.0)
    groups = max(1, rows // 128)
    ssq[...] = jnp.concatenate(
        [jnp.sum(spread[g * 128 : (g + 1) * 128], axis=0, keepdims=True) for g in range(groups)], axis=0
    )

    def y_copy(k, slot):
        to = y_peer(k)
        return pltpu.make_async_remote_copy(
            src_ref=part.at[pl.ds(own * to, own), :, pl.ds(0, cap)], dst_ref=rs.at[slot, :, :, pl.ds(0, cap)],
            send_sem=y_ss.at[k], recv_sem=y_rs.at[k],
            device_id=(ep, to * NX + x), device_id_type=MESH,
        )

    def q_copy(k, slot):
        return pltpu.make_async_remote_copy(
            src_ref=ssq, dst_ref=ssq_all.at[slot],
            send_sem=q_ss.at[k], recv_sem=q_rs.at[k],
            device_id=(ep, y_peer(k) * NX + x), device_id_type=MESH,
        )

    for k in y_steps:
        q_copy(k, y).start()
    blocks = max(1, rows // 128)
    per = rows // blocks

    def gate_up(b, carry):
        at = pl.multiple_of(b * per, per)
        both = dot_nt(xs[pl.ds(at, per), :], wcat[...]).astype(BF16)
        for c in range(2 * half // 128):
            part[pl.ds(b * (per // PAD), per // PAD), c] = both[:, c * 128 : (c + 1) * 128].reshape(
                per // PAD, PAD, 128
            )
        return carry

    lax.fori_loop(0, blocks, gate_up, 0)
    for k in y_steps:
        y_copy(k, y).start()

    ssq_all[y] = ssq[...]

    def y_came(k):
        return lax.rem(y + ny - k, ny)

    for k in y_steps:
        q_copy(k, y_came(k)).wait_recv()
    stats = jnp.sum(ssq_all[...], axis=0)
    mine = own * PAD
    lane = lax.broadcasted_iota(jnp.int32, (mine, 128), 1)
    row = lax.broadcasted_iota(jnp.int32, (mine, 128), 0) + y * mine
    picked = jnp.zeros((mine, 128), F32)
    for g in range(groups):
        picked += jnp.where(row == lane + g * 128, stats[g : g + 1, :], 0.0)
    mean = jnp.sum(picked, axis=1, keepdims=True) / (feats * NX * ny)
    inverse = lax.rsqrt(mean + EPSILON)

    for k in y_steps:
        y_copy(k, y_came(k)).wait_recv()

    def summed(c):
        total = part[pl.ds(own * y, own), c].reshape(mine, 128).astype(F32)
        for k in range(1, ny):
            total += rs[y_came(k), :, c].reshape(mine, 128).astype(F32)
        return total * inverse

    tiles = half // 128
    for c in range(tiles):
        gate_act, up_act = summed(c), summed(tiles + c)
        hidden = (gate_act / (1.0 + jnp.exp(-gate_act)) * up_act).astype(BF16)
        hid[pl.ds(own * y, own), c] = hidden.reshape(own, PAD, 128)

    def h_copy(k, slot):
        return pltpu.make_async_remote_copy(
            src_ref=hid.at[pl.ds(own * slot, own), :, pl.ds(0, cap)],
            dst_ref=hid.at[pl.ds(own * slot, own), :, pl.ds(0, cap)],
            send_sem=h_ss.at[k], recv_sem=h_rs.at[k],
            device_id=(ep, y_peer(k) * NX + x), device_id_type=MESH,
        )

    for k in y_steps:
        h_copy(k, y).start()
    for k in y_steps:
        h_copy(k, y_came(k)).wait_recv()

    def down(b, carry):
        held = jnp.concatenate(
            [hid[pl.ds(b * (per // PAD), per // PAD), c].reshape(per, 128) for c in range(tiles)], axis=1
        )
        piece = dot_nn(held, wdn[...]).astype(BF16)
        for s in range(NX):
            po[s, pl.ds(b * (per // PAD), per // PAD)] = piece[:, s * feats : (s + 1) * feats].reshape(
                per // PAD, PAD, feats
            )
        return carry

    lax.fori_loop(0, blocks, down, 0)

    def o_copy(k, slot):
        return pltpu.make_async_remote_copy(
            src_ref=po.at[x_peer(k), :, pl.ds(0, cap)], dst_ref=xr.at[slot, :, pl.ds(0, cap)],
            send_sem=o_ss.at[k], recv_sem=o_rs.at[k],
            device_id=(ep, y * NX + x_peer(k)), device_id_type=MESH,
        )

    for k in x_steps:
        o_copy(k, x).start()
    xr[x] = po[x]
    for k in x_steps:
        o_copy(k, came(k)).wait_recv()
    for e in range(2):
        back[e] = (xr[2 * e].astype(F32) + xr[2 * e + 1].astype(F32)).astype(BF16)

    def r_copy(peer, slot):
        return pltpu.make_async_remote_copy(
            src_ref=back.at[:, peer, pl.ds(0, cap)],
            dst_ref=ret.at[pl.ds(2 * slot, 2), pl.ds(0, cap)],
            send_sem=r_ss.at[peer], recv_sem=r_rs.at[slot],
            device_id=(peer, tp), device_id_type=MESH,
        )

    each_z(lambda peer: r_copy(peer, ep).start())
    for e in range(2):
        ret[2 * ep + e, 0:cap] = back[e, ep, 0:cap]
    each_z(lambda peer: r_copy(peer, peer).wait_recv())

    answers = ret[...].reshape(experts * PAD, feats)
    p_iota = lax.broadcasted_iota(jnp.int32, (toks, experts * PAD), 1).astype(F32)
    mixed = jnp.zeros((toks, feats), F32)
    for k in range(2):
        pick = jnp.where(p_iota == tcol[:, k : k + 1], 1.0, 0.0).astype(BF16)
        mixed += dot_nn(pick, answers) * tcol[:, 2 + k : 3 + k]
    out_ref[...] = mixed.astype(BF16)

    each_z(lambda peer: z_copy(peer).wait_send())
    each_z(lambda peer: r_copy(peer, ep).wait_send())
    for k in x_steps:
        g_copy(k, x).wait_send()
        for n, ref in weights:
            w_copy(n, ref, k, x).wait_send()
        x_copy(k, x).wait_send()
        o_copy(k, x).wait_send()
    for k in y_steps:
        q_copy(k, y).wait_send()
        y_copy(k, y).wait_send()
        h_copy(k, y).wait_send()


def layer(n_ep, n_tp, tokens, norm_gain, route_ids, route_gates, w_gate, w_up, w_down):
    toks, feats = tokens.shape
    ny = n_tp // NX
    experts = 2 * n_ep
    cap = max(2, (5 * toks * 2 + 4 * experts - 1) // (4 * experts))
    half = w_gate.shape[1] // 2
    own = n_ep // ny
    rows = n_ep * PAD
    groups = max(1, rows // 128)
    dma = pltpu.SemaphoreType.DMA
    vmem = pl.BlockSpec(memory_space=pltpu.VMEM)
    hbm = pl.BlockSpec(memory_space=pl.ANY)
    return pl.pallas_call(
        functools.partial(kernel, n_ep, ny, cap),
        out_shape=jax.ShapeDtypeStruct((toks, feats), BF16),
        in_specs=[vmem, vmem, vmem, vmem, hbm, hbm, hbm],
        out_specs=vmem,
        scratch_shapes=[
            pltpu.VMEM((experts, PAD, feats), BF16),
            pltpu.VMEM((2, n_ep, PAD, feats), BF16),
            pltpu.VMEM((NX, n_ep, PAD, feats), BF16),
            pltpu.VMEM((3, NX, half, feats), BF16),
            pltpu.VMEM((2 * half, NX * feats), BF16),
            pltpu.VMEM((half, NX * feats), BF16),
            pltpu.VMEM((NX, 1, feats), F32),
            pltpu.VMEM((rows, NX * feats), BF16),
            pltpu.VMEM((n_ep, 2 * half // 128, PAD, 128), BF16),
            pltpu.VMEM((ny, own, 2 * half // 128, PAD, 128), BF16),
            pltpu.VMEM((groups, 128), F32),
            pltpu.VMEM((ny, groups, 128), F32),
            pltpu.VMEM((n_ep, half // 128, PAD, 128), BF16),
            pltpu.VMEM((NX, n_ep, PAD, feats), BF16),
            pltpu.VMEM((NX, n_ep, PAD, feats), BF16),
            pltpu.VMEM((2, n_ep, PAD, feats), BF16),
            pltpu.VMEM((experts, PAD, feats), BF16),
            pltpu.VMEM((toks, 128), F32),
            dma((n_ep,)), dma((n_ep,)), dma((n_ep,)), dma((n_ep,)),
            dma((3, NX)), dma((3, NX)), dma((NX,)), dma((NX,)), dma((NX,)), dma((NX,)),
            dma((ny,)), dma((ny,)), dma((ny,)), dma((ny,)), dma((ny,)), dma((ny,)),
            dma((NX,)), dma((NX,)), dma((3,)),
        ],
        compiler_params=pltpu.CompilerParams(collective_id=0, has_side_effects=True),
        name="routed_layer",
    )(tokens, norm_gain.reshape(1, feats), route_ids.T, route_gates.T, w_gate, w_up, w_down)


def solution(mesh):
    placed = (
        P("ep", "tp"),
        P("tp"),
        P("ep", None),
        P("ep", None),
        P("ep", None, "tp"),
        P("ep", None, "tp"),
        P("ep", None, "tp"),
    )
    body = functools.partial(layer, mesh.shape["ep"], mesh.shape["tp"])
    return jax.shard_map(body, mesh=mesh, in_specs=placed, out_specs=P("ep", "tp"), check_vma=False)
```

```python
import functools

import jax
import jax.numpy as jnp
from jax import lax
from jax.experimental import pallas as pl
from jax.experimental.pallas import tpu as pltpu
from jax.sharding import PartitionSpec as P

EPSILON = 1e-06
NX = 4
PAD = 16
CHUNKS = 2
MESH = pl.DeviceIdType.MESH
F32 = jnp.float32
BF16 = jnp.bfloat16


def dot_nt(a, b):
    return lax.dot_general(a, b, (((1,), (1,)), ((), ())), preferred_element_type=F32)


def dot_nn(a, b):
    return lax.dot_general(a, b, (((1,), (0,)), ((), ())), preferred_element_type=F32)


def kernel(
    n_ep, ny, cap,
    tok_hbm, gain_hbm, ids_hbm, gates_hbm, wg_ref, wu_ref, wd_ref,
    out_ref,
    tok, gain, ids_v, gates,
    zsend, zrecv, xg, wland, wcat, wdn, gain_all, xs, part, chain, run, ssq, ssq_all,
    hid, po, xr, back, ret, tcol, mixed_v,
    z_ss, z_rs, r_ss, r_rs, w_ss, w_rs, g_ss, g_rs, x_ss, x_rs,
    y_ss, y_rs, q_ss, q_rs, h_ss, h_rs, o_ss, o_rs, l_sem, i_sem,
):
    nz = n_ep // 2
    rows = n_ep * PAD
    own = n_ep // ny
    oc = own // CHUNKS
    toks, feats = tok.shape
    experts = 2 * n_ep
    half = wg_ref.shape[1] // 2
    tiles = half // 128
    ep = lax.axis_index("ep")
    tp = lax.axis_index("tp")
    z, core = ep // 2, lax.rem(ep, 2)
    y, x = tp // NX, lax.rem(tp, NX)

    def z_peer(i):
        j, c = i // 2, lax.rem(i, 2)
        dz = nz // 2 + (1 - 2 * lax.rem(j, 2)) * ((j + 1) // 2)
        return 2 * lax.rem(z + dz, nz) + c

    def x_peer(k):
        return lax.rem(x + k, NX)

    def y_peer(k):
        return lax.rem(y + k, ny)

    def x_from(k):
        return lax.rem(x + NX - k, NX)

    def y_from(k):
        return lax.rem(y + ny - k, ny)

    def on_x(to):
        return dict(device_id=(ep, y * NX + to), device_id_type=MESH)

    def on_y(to):
        return dict(device_id=(ep, to * NX + x), device_id_type=MESH)

    def on_z(to):
        return dict(device_id=(to, tp), device_id_type=MESH)

    partner = z * 2 + (1 - core)
    x_steps = (2, 1, 3)
    y_steps = sorted(range(1, ny), key=lambda k: -min(k, ny - k))
    far = 2 * (nz - 1)

    barrier = pltpu.get_barrier_semaphore()

    def greet(i, carry):
        pl.semaphore_signal(barrier, inc=1, **on_z(z_peer(i)))
        return carry

    lax.fori_loop(0, far, greet, 0)
    pl.semaphore_signal(barrier, inc=1, **on_z(partner))
    for k in x_steps:
        pl.semaphore_signal(barrier, inc=1, **on_x(x_peer(k)))
    for k in y_steps:
        pl.semaphore_signal(barrier, inc=1, **on_y(y_peer(k)))

    loads = [
        pltpu.make_async_copy(a, b, i_sem.at[n])
        for n, (a, b) in enumerate(((ids_hbm, ids_v), (tok_hbm, tok), (gain_hbm, gain), (gates_hbm, gates)))
    ]
    for load in loads:
        load.start()

    def w_src(ref, to):
        return ref.at[to // 2, pl.ds(lax.rem(to, 2) * half, half), :]

    weights = (wg_ref, wu_ref, wd_ref)
    own_w = [pltpu.make_async_copy(w_src(ref, x), wland.at[n, x], l_sem.at[n]) for n, ref in enumerate(weights)]
    for copy in own_w:
        copy.start()
    ret[...] = jnp.zeros_like(ret)
    for load in loads:
        load.wait()

    ids = ids_v[...].astype(F32)
    e_iota = lax.broadcasted_iota(jnp.int32, (experts, toks), 0).astype(F32)
    m0, m1 = e_iota == ids[0:1, :], e_iota == ids[1:2, :]
    named = jnp.where(m0 | m1, 1.0, 0.0).astype(BF16)
    t_row = lax.broadcasted_iota(jnp.int32, (toks, toks), 0)
    t_col = lax.broadcasted_iota(jnp.int32, (toks, toks), 1)
    earlier = jnp.where(t_row < t_col, 1.0, 0.0).astype(BF16)
    before = dot_nn(named, earlier)
    target0 = ids[0:1, :] * PAD + jnp.sum(jnp.where(m0, before, 0.0), axis=0, keepdims=True)
    target1 = ids[1:2, :] * PAD + jnp.sum(jnp.where(m1, before, 0.0), axis=0, keepdims=True)
    chunk = min(256, experts * PAD)
    for n in range(experts * PAD // chunk):
        p_iota = (lax.broadcasted_iota(jnp.int32, (chunk, toks), 0) + n * chunk).astype(F32)
        pick = jnp.where((p_iota == target0) | (p_iota == target1), 1.0, 0.0).astype(BF16)
        block = dot_nn(pick, tok[...]).astype(BF16)
        zsend[pl.ds(n * chunk // PAD, chunk // PAD)] = block.reshape(chunk // PAD, PAD, feats)
    gain_all[x] = gain[...]

    pl.semaphore_wait(barrier, 2 * nz - 1 + (NX - 1) + (ny - 1))

    def z_copy(peer, slot):
        return pltpu.make_async_remote_copy(
            src_ref=zsend.at[pl.ds(2 * peer, 2), pl.ds(0, cap)], dst_ref=zrecv.at[:, slot, pl.ds(0, cap)],
            send_sem=z_ss, recv_sem=z_rs.at[slot], **on_z(peer),
        )

    def z_start(i, carry):
        z_copy(z_peer(i), ep).start()
        return carry

    lax.fori_loop(0, far, z_start, 0)
    z_copy(partner, ep).start()

    def w_copy(n, k, slot):
        return pltpu.make_async_remote_copy(
            src_ref=w_src(weights[n], x_peer(k)), dst_ref=wland.at[n, slot],
            send_sem=w_ss.at[n, k], recv_sem=w_rs.at[n, k], **on_x(x_peer(k)),
        )

    def g_copy(k, slot):
        return pltpu.make_async_remote_copy(
            src_ref=gain, dst_ref=gain_all.at[slot], send_sem=g_ss.at[k], recv_sem=g_rs.at[k], **on_x(x_peer(k))
        )

    for k in x_steps:
        g_copy(k, x).start()
    for n in range(2):
        for k in x_steps:
            w_copy(n, k, x).start()

    pad_rows = jnp.zeros((124, toks), F32)
    tcol[...] = jnp.concatenate([target0, target1, gates[...], pad_rows], axis=0).T

    def pass_on(src, s):
        for k in x_steps:
            pltpu.make_async_remote_copy(
                src_ref=src(x_peer(k) // 2), dst_ref=xg.at[x, s, pl.ds(0, cap)],
                send_sem=x_ss.at[k], recv_sem=x_rs.at[k], **on_x(x_peer(k)),
            ).start()

    def arrive(s):
        z_copy(s, s).wait_recv()
        pass_on(lambda e: zrecv.at[e, s, pl.ds(0, cap)], s)

    def z_arrive(i, carry):
        arrive(z_peer(far - 1 - i))
        return carry

    pass_on(lambda e: zsend.at[2 * ep + e, pl.ds(0, cap)], ep)
    arrive(partner)
    lax.fori_loop(0, far, z_arrive, 0)
    for k in x_steps:
        w_copy(2, k, x).start()
    xg[x] = zrecv[x // 2]
    xg[x, ep] = zsend[2 * ep + x // 2]

    for n in range(2):
        own_w[n].wait()
    for k in x_steps:
        g_copy(k, x_from(k)).wait_recv()
        for n in range(2):
            w_copy(n, k, x_from(k)).wait_recv()
    for s in range(NX):
        wcat[0:half, s * feats : (s + 1) * feats] = wland[0, s]
        wcat[half : 2 * half, s * feats : (s + 1) * feats] = wland[1, s]

    def x_all(k, slot):
        return pltpu.make_async_remote_copy(
            src_ref=zrecv.at[0, :, pl.ds(0, cap)], dst_ref=xg.at[slot, :, pl.ds(0, cap)],
            send_sem=x_ss.at[k], recv_sem=x_rs.at[k], **on_x(x_peer(k)),
        )

    for k in x_steps:
        x_all(k, x_from(k)).wait_recv()

    squares = jnp.zeros((rows, feats), F32)
    for s in range(NX):
        raw = xg[s].reshape(rows, feats).astype(F32)
        squares += raw * raw
        xs[:, :, s * feats : (s + 1) * feats] = (raw * gain_all[s]).astype(BF16).reshape(ny, own * PAD, feats)
    sums = jnp.sum(squares, axis=1, keepdims=True)
    lane = lax.broadcasted_iota(jnp.int32, (rows, 128), 1)
    row = lax.broadcasted_iota(jnp.int32, (rows, 128), 0)
    spread = jnp.where(lane == lax.rem(row, 128), sums, 0.0)
    groups = max(1, rows // 128)
    ssq[...] = jnp.concatenate(
        [jnp.sum(spread[g * 128 : (g + 1) * 128], axis=0, keepdims=True) for g in range(groups)], axis=0
    )

    def q_copy(k, slot):
        return pltpu.make_async_remote_copy(
            src_ref=ssq, dst_ref=ssq_all.at[slot], send_sem=q_ss.at[k], recv_sem=q_rs.at[k], **on_y(y_peer(k))
        )

    longest = ny // 2

    def length(c, way):
        return longest if (c + way) % 2 == 0 else ny - 1 - longest

    def target_of(c, way, s):
        ahead = length(c, way) - s + 1
        return y_peer(ahead) if way == 0 else y_from(ahead)

    def y_copy(c, way, s):
        to = y_peer(1) if way == 0 else y_from(1)
        if s == 1:
            src = part.at[target_of(c, way, s), pl.ds(c * oc, oc), :, pl.ds(0, cap)]
        else:
            src = run.at[way, c, s - 2, :, :, pl.ds(0, cap)]
        return pltpu.make_async_remote_copy(
            src_ref=src, dst_ref=chain.at[way, c, s - 1, :, :, pl.ds(0, cap)],
            send_sem=y_ss.at[way, c, s - 1], recv_sem=y_rs.at[way, c, s - 1], **on_y(to),
        )

    mc = ny * oc * PAD
    for c in range(CHUNKS):
        both = dot_nt(xs[:, c * oc * PAD : (c + 1) * oc * PAD, :].reshape(mc, NX * feats), wcat[...]).astype(BF16)
        for t in range(2 * tiles):
            part[:, c * oc : (c + 1) * oc, t] = both[:, t * 128 : (t + 1) * 128].reshape(ny, oc, PAD, 128)
        for way in range(2):
            if length(c, way):
                y_copy(c, way, 1).start()
    for k in y_steps:
        q_copy(k, y).start()
    ssq_all[y] = ssq[...]

    for s in range(2, longest + 1):
        for c in range(CHUNKS):
            for way in range(2):
                if length(c, way) >= s:
                    y_copy(c, way, s - 1).wait_recv()
                    mine = part[target_of(c, way, s), c * oc : (c + 1) * oc].astype(F32)
                    run[way, c, s - 2] = (chain[way, c, s - 2].astype(F32) + mine).astype(BF16)
                    y_copy(c, way, s).start()
        if s == 2:
            for k in y_steps:
                q_copy(k, y_from(k)).wait_recv()
            own_w[2].wait()
            for k in x_steps:
                w_copy(2, k, x_from(k)).wait_recv()
            for n in range(NX):
                wdn[:, n * feats : (n + 1) * feats] = wland[2, n]
    if longest < 2:
        for k in y_steps:
            q_copy(k, y_from(k)).wait_recv()
        own_w[2].wait()
        for k in x_steps:
            w_copy(2, k, x_from(k)).wait_recv()
        for n in range(NX):
            wdn[:, n * feats : (n + 1) * feats] = wland[2, n]

    stats = jnp.sum(ssq_all[...], axis=0)
    owned = own * PAD
    lane = lax.broadcasted_iota(jnp.int32, (owned, 128), 1)
    row = lax.broadcasted_iota(jnp.int32, (owned, 128), 0) + y * owned
    picked = jnp.zeros((owned, 128), F32)
    for g in range(groups):
        picked += jnp.where(row == lane + g * 128, stats[g : g + 1, :], 0.0)
    mean = jnp.sum(picked, axis=1, keepdims=True) / (feats * NX * ny)
    inverse = lax.rsqrt(mean + EPSILON)

    def h_copy(c, k, slot):
        return pltpu.make_async_remote_copy(
            src_ref=hid.at[slot, pl.ds(c * oc, oc), :, pl.ds(0, cap)],
            dst_ref=hid.at[slot, pl.ds(c * oc, oc), :, pl.ds(0, cap)],
            send_sem=h_ss.at[c, k], recv_sem=h_rs.at[c, k], **on_y(y_peer(k)),
        )

    for c in range(CHUNKS):
        ends = [(way, length(c, way)) for way in range(2) if length(c, way)]
        for way, s in ends:
            y_copy(c, way, s).wait_recv()
        inv = inverse[c * oc * PAD : (c + 1) * oc * PAD]

        def summed(t):
            total = part[y, c * oc : (c + 1) * oc, t].reshape(oc * PAD, 128).astype(F32)
            for way, s in ends:
                total += chain[way, c, s - 1, :, t].reshape(oc * PAD, 128).astype(F32)
            return total * inv

        for t in range(tiles):
            gate_act, up_act = summed(t), summed(tiles + t)
            hidden = (gate_act / (1.0 + jnp.exp(-gate_act)) * up_act).astype(BF16)
            hid[y, c * oc : (c + 1) * oc, t] = hidden.reshape(oc, PAD, 128)
        for k in y_steps:
            h_copy(c, k, y).start()

    def o_copy(c, k, slot):
        return pltpu.make_async_remote_copy(
            src_ref=po.at[x_peer(k), :, pl.ds(c * oc, oc), pl.ds(0, cap)],
            dst_ref=xr.at[slot, :, pl.ds(c * oc, oc), pl.ds(0, cap)],
            send_sem=o_ss.at[c, k], recv_sem=o_rs.at[c, k], **on_x(x_peer(k)),
        )

    for c in range(CHUNKS):
        for k in y_steps:
            h_copy(c, k, y_from(k)).wait_recv()
        held = jnp.concatenate(
            [hid[:, c * oc : (c + 1) * oc, t].reshape(mc, 128) for t in range(tiles)], axis=1
        )
        piece = dot_nn(held, wdn[...]).astype(BF16)
        for s in range(NX):
            po[s, :, c * oc : (c + 1) * oc] = piece[:, s * feats : (s + 1) * feats].reshape(ny, oc, PAD, feats)
        for k in x_steps:
            o_copy(c, k, x).start()
        xr[x, :, c * oc : (c + 1) * oc] = po[x, :, c * oc : (c + 1) * oc]

    def r_copy(s, slot):
        return pltpu.make_async_remote_copy(
            src_ref=back.at[:, s // own, lax.rem(s, own), pl.ds(0, cap)],
            dst_ref=ret.at[pl.ds(2 * slot, 2), pl.ds(0, cap)],
            send_sem=r_ss, recv_sem=r_rs, **on_z(s),
        )

    group = ep // own
    for c in range(CHUNKS):
        for k in x_steps:
            o_copy(c, k, x_from(k)).wait_recv()
        for e in range(2):
            a, b = (xr[2 * e + n, :, c * oc : (c + 1) * oc].astype(F32) for n in range(2))
            back[e, :, c * oc : (c + 1) * oc] = (a + b).astype(BF16)

        def r_start(i, carry):
            m, at = i // oc, lax.rem(i, oc)
            d = ny // 2 + (1 - 2 * lax.rem(m, 2)) * ((m + 1) // 2)
            s = own * lax.rem(group + d, ny) + c * oc + at

            @pl.when(s != ep)
            def _():
                r_copy(s, ep).start()

            return carry

        lax.fori_loop(0, ny * oc, r_start, 0)
    for e in range(2):
        ret[2 * ep + e, 0:cap] = back[e, group, lax.rem(ep, own), 0:cap]

    for k in x_steps:
        g_copy(k, x).wait_send()
        for n in range(3):
            w_copy(n, k, x).wait_send()
        x_all(k, x).wait_send()
    for k in y_steps:
        q_copy(k, y).wait_send()
        for c in range(CHUNKS):
            h_copy(c, k, y).wait_send()
    for c in range(CHUNKS):
        for way in range(2):
            for s in range(1, length(c, way) + 1):
                y_copy(c, way, s).wait_send()
        for k in x_steps:
            o_copy(c, k, x).wait_send()
    everyone = pl.ds(0, 2 * (n_ep - 1))
    pltpu.make_async_copy(
        zsend.at[everyone, pl.ds(0, cap)], zsend.at[everyone, pl.ds(0, cap)], z_ss
    ).wait()

    pltpu.make_async_copy(ret.at[everyone, pl.ds(0, cap)], ret.at[everyone, pl.ds(0, cap)], r_rs).wait()
    answers = ret[...].reshape(experts * PAD, feats)
    p_iota = lax.broadcasted_iota(jnp.int32, (toks, experts * PAD), 1).astype(F32)
    mixed = jnp.zeros((toks, feats), F32)
    for k in range(2):
        pick = jnp.where(p_iota == tcol[:, k : k + 1], 1.0, 0.0).astype(BF16)
        mixed += dot_nn(pick, answers) * tcol[:, 2 + k : 3 + k]
    mixed_v[...] = mixed.astype(BF16)
    write = pltpu.make_async_copy(mixed_v, out_ref, i_sem.at[0])
    write.start()
    pltpu.make_async_copy(ret.at[everyone, pl.ds(0, cap)], ret.at[everyone, pl.ds(0, cap)], r_ss).wait()
    write.wait()


def layer(n_ep, n_tp, tokens, norm_gain, route_ids, route_gates, w_gate, w_up, w_down):
    toks, feats = tokens.shape
    ny = n_tp // NX
    experts = 2 * n_ep
    cap = max(2, (5 * toks * 2 + 4 * experts - 1) // (4 * experts))
    half = w_gate.shape[1] // 2
    tiles = half // 128
    own = n_ep // ny
    oc = own // CHUNKS
    rows = n_ep * PAD
    groups = max(1, rows // 128)
    hops = ny // 2
    dma = pltpu.SemaphoreType.DMA
    hbm = pl.BlockSpec(memory_space=pl.ANY)
    return pl.pallas_call(
        functools.partial(kernel, n_ep, ny, cap),
        out_shape=jax.ShapeDtypeStruct((toks, feats), BF16),
        in_specs=[hbm] * 7,
        out_specs=hbm,
        scratch_shapes=[
            pltpu.VMEM((toks, feats), BF16),
            pltpu.VMEM((1, feats), F32),
            pltpu.VMEM((2, toks), jnp.int32),
            pltpu.VMEM((2, toks), F32),
            pltpu.VMEM((experts, PAD, feats), BF16),
            pltpu.VMEM((2, n_ep, PAD, feats), BF16),
            pltpu.VMEM((NX, n_ep, PAD, feats), BF16),
            pltpu.VMEM((3, NX, half, feats), BF16),
            pltpu.VMEM((2 * half, NX * feats), BF16),
            pltpu.VMEM((half, NX * feats), BF16),
            pltpu.VMEM((NX, 1, feats), F32),
            pltpu.VMEM((ny, own * PAD, NX * feats), BF16),
            pltpu.VMEM((ny, own, 2 * tiles, PAD, 128), BF16),
            pltpu.VMEM((2, CHUNKS, hops, oc, 2 * tiles, PAD, 128), BF16),
            pltpu.VMEM((2, CHUNKS, max(1, hops - 1), oc, 2 * tiles, PAD, 128), BF16),
            pltpu.VMEM((groups, 128), F32),
            pltpu.VMEM((ny, groups, 128), F32),
            pltpu.VMEM((ny, own, tiles, PAD, 128), BF16),
            pltpu.VMEM((NX, ny, own, PAD, feats), BF16),
            pltpu.VMEM((NX, ny, own, PAD, feats), BF16),
            pltpu.VMEM((2, ny, own, PAD, feats), BF16),
            pltpu.VMEM((experts, PAD, feats), BF16),
            pltpu.VMEM((toks, 128), F32),
            pltpu.VMEM((toks, feats), BF16),
            dma, dma((n_ep,)), dma, dma,
            dma((3, NX)), dma((3, NX)), dma((NX,)), dma((NX,)), dma((NX,)), dma((NX,)),
            dma((2, CHUNKS, hops)), dma((2, CHUNKS, hops)), dma((ny,)), dma((ny,)),
            dma((CHUNKS, ny)), dma((CHUNKS, ny)), dma((CHUNKS, NX)), dma((CHUNKS, NX)), dma((3,)), dma((4,)),
        ],
        compiler_params=pltpu.CompilerParams(collective_id=0, has_side_effects=True),
        name="routed_layer",
    )(tokens, norm_gain.reshape(1, feats), route_ids.T, route_gates.T, w_gate, w_up, w_down)


def solution(mesh):
    placed = (
        P("ep", "tp"),
        P("tp"),
        P("ep", None),
        P("ep", None),
        P("ep", None, "tp"),
        P("ep", None, "tp"),
        P("ep", None, "tp"),
    )
    body = functools.partial(layer, mesh.shape["ep"], mesh.shape["tp"])
    return jax.shard_map(body, mesh=mesh, in_specs=placed, out_specs=P("ep", "tp"), check_vma=False)
```

```python
import functools

import jax
import jax.numpy as jnp
from jax import lax
from jax.experimental import pallas as pl
from jax.experimental.pallas import tpu as pltpu
from jax.sharding import PartitionSpec as P

EPSILON = 1e-06
NX = 4
PAD = 16
MESH = pl.DeviceIdType.MESH
F32 = jnp.float32
BF16 = jnp.bfloat16


def dot_nt(a, b):
    return lax.dot_general(a, b, (((1,), (1,)), ((), ())), preferred_element_type=F32)


def dot_nn(a, b):
    return lax.dot_general(a, b, (((1,), (0,)), ((), ())), preferred_element_type=F32)


def kernel(
    n_ep, ny, cap,
    tok_hbm, gain_hbm, ids_hbm, gates_hbm, wg_ref, wu_ref, wd_ref,
    out_ref,
    tok, gain, ids_v, gates,
    zsend, zrecv, xg, wland, wcat, wdn, gain_all, xs, part, direct, ssq, ssq_all,
    hid, po, xr, back, ret, tcol, picks,
    z_ss, z_rs, r_ss, r_rs, w_ss, w_rs, g_ss, g_rs, x_ss, x_rs,
    d_ss, d_rs, q_ss, q_rs, h_ss, h_rs, o_ss, o_rs, l_sem, i_sem,
):
    nz = n_ep // 2
    chunks = n_ep // ny
    rows = ny * PAD
    toks, feats = tok.shape
    experts = 2 * n_ep
    half = wg_ref.shape[1] // 2
    tiles = half // 128
    ep = lax.axis_index("ep")
    tp = lax.axis_index("tp")
    z, core = ep // 2, lax.rem(ep, 2)
    y, x = tp // NX, lax.rem(tp, NX)
    filled = pl.ds(0, cap)

    def z_peer(i):
        j, c = i // 2, lax.rem(i, 2)
        dz = nz // 2 + (1 - 2 * lax.rem(j, 2)) * ((j + 1) // 2)
        return 2 * lax.rem(z + dz, nz) + c

    def x_peer(k):
        return lax.rem(x + k, NX)

    def y_peer(k):
        return lax.rem(y + k, ny)

    def on_x(k):
        return dict(device_id=(ep, y * NX + x_peer(k)), device_id_type=MESH)

    def on_y(k):
        return dict(device_id=(ep, y_peer(k) * NX + x), device_id_type=MESH)

    def on_z(to):
        return dict(device_id=(to, tp), device_id_type=MESH)

    def settle(ref, sem):
        pltpu.make_async_copy(ref, ref, sem).wait()

    partner = z * 2 + (1 - core)
    x_steps = (2, 1, 3)
    y_steps = sorted(range(1, ny), key=lambda k: -min(k, ny - k))
    far = 2 * (nz - 1)

    barrier = pltpu.get_barrier_semaphore()

    def greet(i, carry):
        pl.semaphore_signal(barrier, inc=1, **on_z(z_peer(i)))
        return carry

    lax.fori_loop(0, far, greet, 0)
    pl.semaphore_signal(barrier, inc=1, **on_z(partner))
    for k in x_steps:
        pl.semaphore_signal(barrier, inc=1, **on_x(k))
    for k in y_steps:
        pl.semaphore_signal(barrier, inc=1, **on_y(k))

    loads = [
        pltpu.make_async_copy(a, b, i_sem.at[n])
        for n, (a, b) in enumerate(((ids_hbm, ids_v), (tok_hbm, tok), (gain_hbm, gain), (gates_hbm, gates)))
    ]
    for load in loads:
        load.start()

    def w_src(ref, to):
        return ref.at[to // 2, pl.ds(lax.rem(to, 2) * half, half), :]

    weights = (wg_ref, wu_ref, wd_ref)
    for n, ref in enumerate(weights):
        pltpu.make_async_copy(w_src(ref, x), wland.at[n, x], l_sem).start()
    ret[...] = jnp.zeros_like(ret)
    for load in loads:
        load.wait()

    ids = ids_v[...].astype(F32)
    e_iota = lax.broadcasted_iota(jnp.int32, (experts, toks), 0).astype(F32)
    m0, m1 = e_iota == ids[0:1, :], e_iota == ids[1:2, :]
    named = jnp.where(m0 | m1, 1.0, 0.0).astype(BF16)
    t_row = lax.broadcasted_iota(jnp.int32, (toks, toks), 0)
    t_col = lax.broadcasted_iota(jnp.int32, (toks, toks), 1)
    earlier = jnp.where(t_row < t_col, 1.0, 0.0).astype(BF16)
    before = dot_nn(named, earlier)
    target0 = ids[0:1, :] * PAD + jnp.sum(jnp.where(m0, before, 0.0), axis=0, keepdims=True)
    target1 = ids[1:2, :] * PAD + jnp.sum(jnp.where(m1, before, 0.0), axis=0, keepdims=True)
    size = min(256, experts * PAD)
    for n in range(experts * PAD // size):
        p_iota = (lax.broadcasted_iota(jnp.int32, (size, toks), 0) + n * size).astype(F32)
        pick = jnp.where((p_iota == target0) | (p_iota == target1), 1.0, 0.0).astype(BF16)
        block = dot_nn(pick, tok[...]).astype(BF16)
        zsend[pl.ds(n * size // PAD, size // PAD)] = block.reshape(size // PAD, PAD, feats)
    gain_all[x] = gain[...]

    pl.semaphore_wait(barrier, 2 * nz - 1 + (NX - 1) + (ny - 1))

    def z_copy(peer):
        return pltpu.make_async_remote_copy(
            src_ref=zsend.at[pl.ds(2 * peer, 2), filled], dst_ref=zrecv.at[:, ep, filled],
            send_sem=z_ss, recv_sem=z_rs.at[ep // ny], **on_z(peer),
        )

    def z_start(i, carry):
        z_copy(z_peer(i)).start()
        return carry

    lax.fori_loop(0, far, z_start, 0)
    z_copy(partner).start()

    def send_weight(n):
        for k in x_steps:
            pltpu.make_async_remote_copy(
                src_ref=w_src(weights[n], x_peer(k)), dst_ref=wland.at[n, x],
                send_sem=w_ss, recv_sem=w_rs.at[n], **on_x(k),
            ).start()

    for k in x_steps:
        pltpu.make_async_remote_copy(
            src_ref=gain, dst_ref=gain_all.at[x], send_sem=g_ss, recv_sem=g_rs, **on_x(k)
        ).start()
    send_weight(0)
    send_weight(1)
    for e in range(2):
        zrecv[e, ep] = zsend[2 * ep + e]

    pad_rows = jnp.zeros((124, toks), F32)
    tcol[...] = jnp.concatenate([target0, target1, gates[...], pad_rows], axis=0).T

    def arrive(c):
        @pl.when(ep // ny == c)
        def _():
            settle(zrecv.at[:, pl.ds(0, ny - 1), filled], z_rs.at[c])

        @pl.when(ep // ny != c)
        def _():
            settle(zrecv.at[:, pl.ds(0, ny), filled], z_rs.at[c])

        for k in x_steps:
            pltpu.make_async_remote_copy(
                src_ref=zrecv.at[x_peer(k) // 2, pl.ds(c * ny, ny), filled],
                dst_ref=xg.at[x, pl.ds(c * ny, ny), filled],
                send_sem=x_ss, recv_sem=x_rs.at[c], **on_x(k),
            ).start()
        xg[x, c * ny : (c + 1) * ny] = zrecv[x // 2, c * ny : (c + 1) * ny]

    lane = lax.broadcasted_iota(jnp.int32, (rows, 128), 1)
    row = lax.broadcasted_iota(jnp.int32, (rows, 128), 0)

    def gate_up(c):
        settle(xg.at[pl.ds(0, NX - 1), pl.ds(0, ny), filled], x_rs.at[c])
        squares = jnp.zeros((rows, feats), F32)
        for s in range(NX):
            raw = xg[s, c * ny : (c + 1) * ny].reshape(rows, feats).astype(F32)
            squares += raw * raw
            xs[:, s * feats : (s + 1) * feats] = (raw * gain_all[s]).astype(BF16)
        both = dot_nt(xs[...], wcat[...]).astype(BF16)
        for t in range(2 * tiles):
            part[c, :, t] = both[:, t * 128 : (t + 1) * 128].reshape(ny, PAD, 128)
        for k in y_steps:
            pltpu.make_async_remote_copy(
                src_ref=part.at[c, y_peer(k), :, filled], dst_ref=direct.at[c, k - 1, :, filled],
                send_sem=d_ss, recv_sem=d_rs.at[c], **on_y(k),
            ).start()
        sums = jnp.sum(squares, axis=1, keepdims=True)
        ssq[c] = jnp.sum(jnp.where(lane == row, sums, 0.0), axis=0, keepdims=True)
        for k in y_steps:
            pltpu.make_async_remote_copy(
                src_ref=ssq.at[c], dst_ref=ssq_all.at[c, k - 1], send_sem=q_ss, recv_sem=q_rs.at[c], **on_y(k)
            ).start()

    def activate(c):
        settle(ssq_all.at[c, pl.ds(0, ny - 1)], q_rs.at[c])
        stats = ssq[c] + jnp.sum(ssq_all[c], axis=0)
        held = jnp.where(row[:PAD] + y * PAD == lane[:PAD], stats, 0.0)
        mean = jnp.sum(held, axis=1, keepdims=True) / (feats * NX * ny)
        inverse = lax.rsqrt(mean + EPSILON)
        settle(direct.at[c, pl.ds(0, ny - 1), :, filled], d_rs.at[c])

        def summed(t):
            total = part[c, y, t].astype(F32)
            for k in range(ny - 1):
                total += direct[c, k, t].astype(F32)
            return total * inverse

        for t in range(tiles):
            gate_act, up_act = summed(t), summed(tiles + t)
            hid[c, y, t] = (gate_act / (1.0 + jnp.exp(-gate_act)) * up_act).astype(BF16)
        for k in y_steps:
            pltpu.make_async_remote_copy(
                src_ref=hid.at[c, y, :, filled], dst_ref=hid.at[c, y, :, filled],
                send_sem=h_ss, recv_sem=h_rs.at[c], **on_y(k),
            ).start()

    def down(c):
        settle(hid.at[c, pl.ds(0, ny - 1), :, filled], h_rs.at[c])
        held = jnp.concatenate([hid[c, :, t].reshape(rows, 128) for t in range(tiles)], axis=1)
        piece = dot_nn(held, wdn[...]).astype(BF16)
        for s in range(NX):
            po[s, c] = piece[:, s * feats : (s + 1) * feats].reshape(ny, PAD, feats)
        for k in x_steps:
            pltpu.make_async_remote_copy(
                src_ref=po.at[x_peer(k), c, :, filled], dst_ref=xr.at[x, c, :, filled],
                send_sem=o_ss, recv_sem=o_rs.at[c], **on_x(k),
            ).start()
        xr[x, c] = po[x, c]

    def r_copy(s):
        return pltpu.make_async_remote_copy(
            src_ref=back.at[:, s, filled], dst_ref=ret.at[pl.ds(2 * ep, 2), filled],
            send_sem=r_ss, recv_sem=r_rs, **on_z(s),
        )

    def give_back(c):
        settle(xr.at[pl.ds(0, NX - 1), 0, :, filled], o_rs.at[c])
        for e in range(2):
            back[e, c * ny : (c + 1) * ny] = (xr[2 * e, c].astype(F32) + xr[2 * e + 1, c].astype(F32)).astype(BF16)

        def r_start(i, carry):
            @pl.when(c * ny + i != ep)
            def _():
                r_copy(c * ny + i).start()

            return carry

        lax.fori_loop(0, ny, r_start, 0)

    def join_gate_up():
        settle(wland.at[:, 0], l_sem)
        settle(gain_all.at[pl.ds(0, NX - 1)], g_rs)
        for n in range(2):
            settle(wland.at[n, pl.ds(0, NX - 1)], w_rs.at[n])
            for s in range(NX):
                wcat[n * half : (n + 1) * half, s * feats : (s + 1) * feats] = wland[n, s]

    def join_down():
        settle(wland.at[2, pl.ds(0, NX - 1)], w_rs.at[2])
        for s in range(NX):
            wdn[:, s * feats : (s + 1) * feats] = wland[2, s]

    ahead = min(2, chunks)
    for c in range(ahead):
        arrive(c)
    join_gate_up()
    for c in range(ahead):
        gate_up(c)
        if c + ahead < chunks:
            arrive(c + ahead)
    send_weight(2)
    p_iota = lax.broadcasted_iota(jnp.int32, (toks, experts * PAD), 1).astype(F32)
    for k in range(2):
        picks[k] = jnp.where(p_iota == tcol[:, k : k + 1], 1.0, 0.0).astype(BF16)
    for c in range(ahead):
        activate(c)
        if c + ahead < chunks:
            gate_up(c + ahead)
    join_down()
    down(0)
    for c in range(chunks):
        if c + ahead < chunks:
            activate(c + ahead)
        if c + 1 < chunks:
            down(c + 1)
        give_back(c)
    for e in range(2):
        ret[2 * ep + e, 0:cap] = back[e, ep, 0:cap]

    settle(zsend.at[pl.ds(0, 2 * (n_ep - 1)), filled], z_ss)
    settle(gain_all.at[pl.ds(0, NX - 1)], g_ss)
    settle(wland.at[:, pl.ds(0, NX - 1)], w_ss)
    settle(xg.at[pl.ds(0, NX - 1), :, filled], x_ss)
    settle(direct.at[:, :, :, filled], d_ss)
    settle(ssq_all, q_ss)
    settle(hid.at[:, pl.ds(0, ny - 1), :, filled], h_ss)
    settle(xr.at[pl.ds(0, NX - 1), :, :, filled], o_ss)

    everyone = ret.at[pl.ds(0, 2 * (n_ep - 1)), filled]
    settle(everyone, r_rs)
    answers = ret[...].reshape(experts * PAD, feats)
    out_ref[...] = (dot_nn(picks[0], answers) * tcol[:, 2:3] + dot_nn(picks[1], answers) * tcol[:, 3:4]).astype(BF16)
    settle(everyone, r_ss)


def layer(n_ep, n_tp, tokens, norm_gain, route_ids, route_gates, w_gate, w_up, w_down):
    toks, feats = tokens.shape
    ny = n_tp // NX
    chunks = n_ep // ny
    experts = 2 * n_ep
    cap = max(2, (5 * toks * 2 + 4 * experts - 1) // (4 * experts))
    half = w_gate.shape[1] // 2
    tiles = half // 128
    dma = pltpu.SemaphoreType.DMA
    each = pltpu.SemaphoreType.DMA((chunks,))
    hbm = pl.BlockSpec(memory_space=pl.ANY)
    mixed = pl.pallas_call(
        functools.partial(kernel, n_ep, ny, cap),
        out_shape=pltpu.VMEM((toks, feats), BF16),
        in_specs=[hbm] * 7,
        out_specs=pl.BlockSpec(memory_space=pltpu.VMEM),
        scratch_shapes=[
            pltpu.VMEM((toks, feats), BF16),
            pltpu.VMEM((1, feats), F32),
            pltpu.VMEM((2, toks), jnp.int32),
            pltpu.VMEM((2, toks), F32),
            pltpu.VMEM((experts, PAD, feats), BF16),
            pltpu.VMEM((2, n_ep, PAD, feats), BF16),
            pltpu.VMEM((NX, n_ep, PAD, feats), BF16),
            pltpu.VMEM((3, NX, half, feats), BF16),
            pltpu.VMEM((2 * half, NX * feats), BF16),
            pltpu.VMEM((half, NX * feats), BF16),
            pltpu.VMEM((NX, 1, feats), F32),
            pltpu.VMEM((ny * PAD, NX * feats), BF16),
            pltpu.VMEM((chunks, ny, 2 * tiles, PAD, 128), BF16),
            pltpu.VMEM((chunks, ny - 1, 2 * tiles, PAD, 128), BF16),
            pltpu.VMEM((chunks, 1, 128), F32),
            pltpu.VMEM((chunks, ny - 1, 1, 128), F32),
            pltpu.VMEM((chunks, ny, tiles, PAD, 128), BF16),
            pltpu.VMEM((NX, chunks, ny, PAD, feats), BF16),
            pltpu.VMEM((NX, chunks, ny, PAD, feats), BF16),
            pltpu.VMEM((2, n_ep, PAD, feats), BF16),
            pltpu.VMEM((experts, PAD, feats), BF16),
            pltpu.VMEM((toks, 128), F32),
            pltpu.VMEM((2, toks, experts * PAD), BF16),
            dma, each, dma, dma, dma, dma((3,)), dma, dma, dma, each,
            dma, each, dma, each, dma, each, dma, each, dma, dma((4,)),
        ],
        compiler_params=pltpu.CompilerParams(collective_id=0, has_side_effects=True),
        name="routed_layer",
    )(tokens, norm_gain.reshape(1, feats), route_ids.T, route_gates.T, w_gate, w_up, w_down)
    return mixed


def solution(mesh):
    placed = (
        P("ep", "tp"),
        P("tp"),
        P("ep", None),
        P("ep", None),
        P("ep", None, "tp"),
        P("ep", None, "tp"),
        P("ep", None, "tp"),
    )
    body = functools.partial(layer, mesh.shape["ep"], mesh.shape["tp"])
    return jax.shard_map(body, mesh=mesh, in_specs=placed, out_specs=P("ep", "tp"), check_vma=False)
```

```python
import functools

import jax
import jax.numpy as jnp
from jax import lax
from jax.experimental import pallas as pl
from jax.experimental.pallas import tpu as pltpu
from jax.sharding import PartitionSpec as P

EPSILON = 1e-06
NX = 4
PAD = 16
MESH = pl.DeviceIdType.MESH
F32 = jnp.float32
BF16 = jnp.bfloat16


def dot_nt(a, b):
    return lax.dot_general(a, b, (((1,), (1,)), ((), ())), preferred_element_type=F32)


def dot_nn(a, b):
    return lax.dot_general(a, b, (((1,), (0,)), ((), ())), preferred_element_type=F32)


def kernel(
    n_ep, ny, cap,
    tok_hbm, gain_hbm, ids_hbm, gates_hbm, wg_ref, wu_ref, wd_ref,
    out_ref,
    tok, gain, ids_v, gates,
    zsend, zrecv, xg, wland, wcat, wdn, gain_all, xs, part, direct, ssq, ssq_all,
    hid, po, xr, back, ret, tcol, picks, staged, chain, run,
    z_ss, z_rs, r_ss, r_rs, w_ss, w_rs, g_ss, g_rs, x_ss, x_rs,
    d_ss, d_rs, q_ss, q_rs, h_ss, h_rs, o_ss, o_rs, l_sem, i_sem, y_ss, y_rs,
):
    nz = n_ep // 2
    chunks = n_ep // ny
    rows = ny * PAD
    toks, feats = tok.shape
    experts = 2 * n_ep
    half = wg_ref.shape[1] // 2
    tiles = half // 128
    ep = lax.axis_index("ep")
    tp = lax.axis_index("tp")
    z, core = ep // 2, lax.rem(ep, 2)
    y, x = tp // NX, lax.rem(tp, NX)
    filled = pl.ds(0, cap)

    def z_peer(i):
        j, c = i // 2, lax.rem(i, 2)
        dz = nz // 2 + (1 - 2 * lax.rem(j, 2)) * ((j + 1) // 2)
        return 2 * lax.rem(z + dz, nz) + c

    side = nz // 2

    def slot_of(s):
        lo = lax.rem(s // 2, side)
        return 2 * (4 * (lo // 2) + 2 * (s // 2 // side) + lax.rem(lo, 2)) + lax.rem(s, 2)

    def source_of(n):
        v = n // 2
        return 2 * (side * lax.rem(v // 2, 2) + 2 * (v // 4) + lax.rem(v, 2)) + lax.rem(n, 2)

    mine = slot_of(ep)

    def x_peer(k):
        return lax.rem(x + k, NX)

    def y_peer(k):
        return lax.rem(y + k, ny)

    def on_x(k):
        return dict(device_id=(ep, y * NX + x_peer(k)), device_id_type=MESH)

    def on_y(k):
        return dict(device_id=(ep, y_peer(k) * NX + x), device_id_type=MESH)

    def on_z(to):
        return dict(device_id=(to, tp), device_id_type=MESH)

    def settle(ref, sem):
        pltpu.make_async_copy(ref, ref, sem).wait()

    partner = z * 2 + (1 - core)
    x_steps = (2, 1, 3)
    y_steps = sorted(range(1, ny), key=lambda k: -min(k, ny - k))
    far = 2 * (nz - 1)

    loads = [
        pltpu.make_async_copy(a, b, i_sem.at[n])
        for n, (a, b) in enumerate(((ids_hbm, ids_v), (tok_hbm, tok), (gain_hbm, gain), (gates_hbm, gates)))
    ]
    for load in loads[:2]:
        load.start()

    barrier = pltpu.get_barrier_semaphore()

    def greet(i, carry):
        pl.semaphore_signal(barrier, inc=1, **on_z(z_peer(i)))
        return carry

    lax.fori_loop(0, far, greet, 0)
    pl.semaphore_signal(barrier, inc=1, **on_z(partner))
    for k in x_steps:
        pl.semaphore_signal(barrier, inc=1, **on_x(k))
    for k in y_steps:
        pl.semaphore_signal(barrier, inc=1, **on_y(k))

    for load in loads[2:]:
        load.start()

    def w_src(n, to):
        return staged.at[n, to // 2, pl.ds(pl.multiple_of(lax.rem(to, 2) * half, half), half)]

    weights = (wg_ref, wu_ref, wd_ref)
    for n, ref in enumerate(weights):
        pltpu.make_async_copy(ref, staged.at[n], l_sem).start()
    ret[...] = jnp.zeros_like(ret)
    for load in loads:
        load.wait()

    ids = ids_v[...].astype(F32)
    e_iota = lax.broadcasted_iota(jnp.int32, (experts, toks), 0).astype(F32)
    m0, m1 = e_iota == ids[0:1, :], e_iota == ids[1:2, :]
    named = jnp.where(m0 | m1, 1.0, 0.0).astype(BF16)
    t_row = lax.broadcasted_iota(jnp.int32, (toks, toks), 0)
    t_col = lax.broadcasted_iota(jnp.int32, (toks, toks), 1)
    earlier = jnp.where(t_row < t_col, 1.0, 0.0).astype(BF16)
    before = dot_nn(named, earlier)
    target0 = ids[0:1, :] * PAD + jnp.sum(jnp.where(m0, before, 0.0), axis=0, keepdims=True)
    target1 = ids[1:2, :] * PAD + jnp.sum(jnp.where(m1, before, 0.0), axis=0, keepdims=True)
    size = min(256, experts * PAD)
    for n in range(experts * PAD // size):
        p_iota = (lax.broadcasted_iota(jnp.int32, (size, toks), 0) + n * size).astype(F32)
        pick = jnp.where((p_iota == target0) | (p_iota == target1), 1.0, 0.0).astype(BF16)
        block = dot_nn(pick, tok[...]).astype(BF16)
        zsend[pl.ds(n * size // PAD, size // PAD)] = block.reshape(size // PAD, PAD, feats)
    gain_all[x] = gain[...]
    pl.semaphore_wait(barrier, 2 * nz - 1 + (NX - 1) + (ny - 1))
    settle(staged, l_sem)

    def z_copy(peer):
        return pltpu.make_async_remote_copy(
            src_ref=zsend.at[pl.ds(2 * peer, 2), filled], dst_ref=zrecv.at[:, mine, filled],
            send_sem=z_ss, recv_sem=z_rs.at[mine // ny], **on_z(peer),
        )

    def z_start(i, carry):
        z_copy(z_peer(i)).start()
        return carry


    def send_weight(n):
        for k in x_steps:
            pltpu.make_async_remote_copy(
                src_ref=w_src(n, x_peer(k)), dst_ref=wland.at[n, x],
                send_sem=w_ss, recv_sem=w_rs.at[n], **on_x(k),
            ).start()

    for k in x_steps:
        pltpu.make_async_remote_copy(
            src_ref=gain, dst_ref=gain_all.at[x], send_sem=g_ss, recv_sem=g_rs, **on_x(k)
        ).start()
    send_weight(0)
    send_weight(1)
    lax.fori_loop(0, far, z_start, 0)
    z_copy(partner).start()
    for e in range(2):
        zrecv[e, mine] = zsend[2 * ep + e]
    for n in range(3):
        wland[n, x] = w_src(n, x)[...]

    pad_rows = jnp.zeros((124, toks), F32)
    tcol[...] = jnp.concatenate([target0, target1, gates[...], pad_rows], axis=0).T

    def arrive(c):
        @pl.when(mine // ny == c)
        def _():
            settle(zrecv.at[:, pl.ds(0, ny - 1), filled], z_rs.at[c])

        @pl.when(mine // ny != c)
        def _():
            settle(zrecv.at[:, pl.ds(0, ny), filled], z_rs.at[c])

        for k in x_steps:
            pltpu.make_async_remote_copy(
                src_ref=zrecv.at[x_peer(k) // 2, pl.ds(c * ny, ny), filled],
                dst_ref=xg.at[x, pl.ds(c * ny, ny), filled],
                send_sem=x_ss, recv_sem=x_rs.at[c], **on_x(k),
            ).start()
        xg[x, c * ny : (c + 1) * ny] = zrecv[x // 2, c * ny : (c + 1) * ny]

    longest = ny // 2
    straight = chunks // 2

    def length(c, way):
        return longest if (c + way) % 2 == 0 else ny - 1 - longest

    def place(c, way, s):
        return s - 1 + (length(c, 0) if way else 0)

    def towards(c, way, s):
        left = length(c, way) - s + 1
        return y_peer(left if way == 0 else ny - left)

    def chain_start(c, way, s):
        n, at = c - straight, place(c, way, s)
        src = part.at[c, towards(c, way, s)] if s == 1 else run.at[n, at]
        pltpu.make_async_remote_copy(
            src_ref=src.at[:, filled], dst_ref=chain.at[n, at, :, filled],
            send_sem=y_ss, recv_sem=y_rs.at[n, at], **on_y(1 if way == 0 else ny - 1),
        ).start()

    def chain_end(c, way, s):
        n, at = c - straight, place(c, way, s)
        settle(chain.at[n, at, :, filled], y_rs.at[n, at])
        return chain.at[n, at]

    def hop(s):
        for c in range(straight, chunks):
            for way in range(2):
                if length(c, way) >= s:
                    came = chain_end(c, way, s - 1)[...].astype(F32)
                    run[c - straight, place(c, way, s)] = (came + part[c, towards(c, way, s)].astype(F32)).astype(BF16)
                    chain_start(c, way, s)

    lane = lax.broadcasted_iota(jnp.int32, (rows, 128), 1)
    row = lax.broadcasted_iota(jnp.int32, (rows, 128), 0)

    def gate_up(c):
        settle(xg.at[pl.ds(0, NX - 1), pl.ds(0, ny), filled], x_rs.at[c])
        squares = jnp.zeros((rows, feats), F32)
        for s in range(NX):
            raw = xg[s, c * ny : (c + 1) * ny].reshape(rows, feats).astype(F32)
            squares += raw * raw
            xs[:, s * feats : (s + 1) * feats] = (raw * gain_all[s]).astype(BF16)
        both = dot_nt(xs[...], wcat[...]).astype(BF16)
        for t in range(2 * tiles):
            part[c, :, t] = both[:, t * 128 : (t + 1) * 128].reshape(ny, PAD, 128)
        sums = jnp.sum(squares, axis=1, keepdims=True)
        ssq[c] = jnp.sum(jnp.where(lane == row, sums, 0.0), axis=0, keepdims=True)

    def send_stats(c):
        for k in y_steps:
            pltpu.make_async_remote_copy(
                src_ref=ssq.at[c], dst_ref=ssq_all.at[c, k - 1], send_sem=q_ss, recv_sem=q_rs.at[c], **on_y(k)
            ).start()

    def send_sums(c):
        for k in y_steps:
            pltpu.make_async_remote_copy(
                src_ref=part.at[c, y_peer(k), :, filled], dst_ref=direct.at[c, k - 1, :, filled],
                send_sem=d_ss, recv_sem=d_rs.at[c], **on_y(k),
            ).start()
        send_stats(c)

    def send_chain(c):
        for way in range(2):
            if length(c, way):
                chain_start(c, way, 1)
        send_stats(c)

    def activate(c, chained=False):
        settle(ssq_all.at[c, pl.ds(0, ny - 1)], q_rs.at[c])
        stats = ssq[c] + jnp.sum(ssq_all[c], axis=0)
        held = jnp.where(row[:PAD] + y * PAD == lane[:PAD], stats, 0.0)
        mean = jnp.sum(held, axis=1, keepdims=True) / (feats * NX * ny)
        inverse = lax.rsqrt(mean + EPSILON)
        if chained:
            terms = [chain_end(c, way, length(c, way)) for way in range(2) if length(c, way)]
        else:
            settle(direct.at[c, pl.ds(0, ny - 1), :, filled], d_rs.at[c])
            terms = [direct.at[c, k] for k in range(ny - 1)]

        def summed(t):
            total = part[c, y, t].astype(F32)
            for term in terms:
                total += term[t].astype(F32)
            return total * inverse

        for t in range(tiles):
            gate_act, up_act = summed(t), summed(tiles + t)
            hid[c, y, t] = (gate_act / (1.0 + jnp.exp(-gate_act)) * up_act).astype(BF16)
        for k in y_steps:
            pltpu.make_async_remote_copy(
                src_ref=hid.at[c, y, :, filled], dst_ref=hid.at[c, y, :, filled],
                send_sem=h_ss, recv_sem=h_rs.at[c], **on_y(k),
            ).start()

    def down(c):
        settle(hid.at[c, pl.ds(0, ny - 1), :, filled], h_rs.at[c])
        held = jnp.concatenate([hid[c, :, t].reshape(rows, 128) for t in range(tiles)], axis=1)
        piece = dot_nn(held, wdn[...]).astype(BF16)
        for s in range(NX):
            po[s, c] = piece[:, s * feats : (s + 1) * feats].reshape(ny, PAD, feats)
        for k in x_steps:
            pltpu.make_async_remote_copy(
                src_ref=po.at[x_peer(k), c, :, filled], dst_ref=xr.at[x, c, :, filled],
                send_sem=o_ss, recv_sem=o_rs.at[c], **on_x(k),
            ).start()
        xr[x, c] = po[x, c]

    def r_copy(n):
        return pltpu.make_async_remote_copy(
            src_ref=back.at[:, n, filled], dst_ref=ret.at[pl.ds(2 * ep, 2), filled],
            send_sem=r_ss, recv_sem=r_rs, **on_z(source_of(n)),
        )

    def give_back(c):
        settle(xr.at[pl.ds(0, NX - 1), 0, :, filled], o_rs.at[c])
        for e in range(2):
            back[e, c * ny : (c + 1) * ny] = (xr[2 * e, c].astype(F32) + xr[2 * e + 1, c].astype(F32)).astype(BF16)

        def r_start(i, carry):
            @pl.when(c * ny + i != mine)
            def _():
                r_copy(c * ny + i).start()

            return carry

        lax.fori_loop(0, ny, r_start, 0)

    def join_gate_up():
        settle(gain_all.at[pl.ds(0, NX - 1)], g_rs)
        for n in range(2):
            settle(wland.at[n, pl.ds(0, NX - 1)], w_rs.at[n])
            for s in range(NX):
                wcat[n * half : (n + 1) * half, s * feats : (s + 1) * feats] = wland[n, s]

    def join_down():
        settle(wland.at[2, pl.ds(0, NX - 1)], w_rs.at[2])
        for s in range(NX):
            wdn[:, s * feats : (s + 1) * feats] = wland[2, s]

    p_iota = lax.broadcasted_iota(jnp.int32, (toks, experts * PAD), 1).astype(F32)
    for k in range(2):
        picks[k * toks : (k + 1) * toks] = jnp.where(p_iota == tcol[:, k : k + 1], 1.0, 0.0).astype(BF16)
    for c in range(min(3, chunks)):
        arrive(c)
    join_gate_up()
    for c in range(chunks):
        gate_up(c)
        if c < straight:
            send_sums(c)
        else:

            @pl.when(core == 1)
            def _():
                send_chain(c)

        if c + 3 < chunks:
            arrive(c + 3)
        if c == straight - 1:
            send_weight(2)

    @pl.when(core == 0)
    def _():
        for c in range(straight):
            activate(c)
            send_sums(c + straight)
        join_down()
        down(0)
        for c in range(chunks):
            if c + straight < chunks:
                activate(c + straight)
            if c + 1 < chunks:
                down(c + 1)
            give_back(c)
        settle(direct.at[:, :, :, filled], d_ss)

    @pl.when(core == 1)
    def _():
        for c in range(straight):
            activate(c)
            if c + 2 <= longest:
                hop(c + 2)
        join_down()
        down(0)
        for s in range(straight + 2, longest + 1):
            hop(s)
        for c in range(1, straight):
            down(c)
        give_back(0)
        for c in range(straight, chunks):
            activate(c, True)
        for c in range(1, straight):
            give_back(c)
        for c in range(straight, chunks):
            down(c)
        for c in range(straight, chunks):
            give_back(c)
        settle(direct.at[pl.ds(0, straight), :, :, filled], d_ss)
        settle(chain.at[:, :, :, filled], y_ss)

    for e in range(2):
        ret[2 * ep + e, 0:cap] = back[e, mine, 0:cap]

    settle(zsend.at[pl.ds(0, 2 * (n_ep - 1)), filled], z_ss)
    settle(gain_all.at[pl.ds(0, NX - 1)], g_ss)
    settle(wland.at[:, pl.ds(0, NX - 1)], w_ss)
    settle(xg.at[pl.ds(0, NX - 1), :, filled], x_ss)
    settle(ssq_all, q_ss)
    settle(hid.at[:, pl.ds(0, ny - 1), :, filled], h_ss)
    settle(xr.at[pl.ds(0, NX - 1), :, :, filled], o_ss)

    everyone = ret.at[pl.ds(0, 2 * (n_ep - 1)), filled]
    settle(everyone, r_rs)
    answers = ret[...].reshape(experts * PAD, feats)
    picked = dot_nn(picks[...], answers)
    out_ref[...] = (picked[:toks] * tcol[:, 2:3] + picked[toks:] * tcol[:, 3:4]).astype(BF16)
    settle(everyone, r_ss)


def layer(n_ep, n_tp, tokens, norm_gain, route_ids, route_gates, w_gate, w_up, w_down):
    toks, feats = tokens.shape
    ny = n_tp // NX
    chunks = n_ep // ny
    experts = 2 * n_ep
    cap = max(2, (5 * toks * 2 + 4 * experts - 1) // (4 * experts))
    half = w_gate.shape[1] // 2
    tiles = half // 128
    dma = pltpu.SemaphoreType.DMA
    each = pltpu.SemaphoreType.DMA((chunks,))
    hbm = pl.BlockSpec(memory_space=pl.ANY)
    mixed = pl.pallas_call(
        functools.partial(kernel, n_ep, ny, cap),
        out_shape=pltpu.VMEM((toks, feats), BF16),
        in_specs=[hbm] * 7,
        out_specs=pl.BlockSpec(memory_space=pltpu.VMEM),
        scratch_shapes=[
            pltpu.VMEM((toks, feats), BF16),
            pltpu.VMEM((1, feats), F32),
            pltpu.VMEM((2, toks), jnp.int32),
            pltpu.VMEM((2, toks), F32),
            pltpu.VMEM((experts, PAD, feats), BF16),
            pltpu.VMEM((2, n_ep, PAD, feats), BF16),
            pltpu.VMEM((NX, n_ep, PAD, feats), BF16),
            pltpu.VMEM((3, NX, half, feats), BF16),
            pltpu.VMEM((2 * half, NX * feats), BF16),
            pltpu.VMEM((half, NX * feats), BF16),
            pltpu.VMEM((NX, 1, feats), F32),
            pltpu.VMEM((ny * PAD, NX * feats), BF16),
            pltpu.VMEM((chunks, ny, 2 * tiles, PAD, 128), BF16),
            pltpu.VMEM((chunks, ny - 1, 2 * tiles, PAD, 128), BF16),
            pltpu.VMEM((chunks, 1, 128), F32),
            pltpu.VMEM((chunks, ny - 1, 1, 128), F32),
            pltpu.VMEM((chunks, ny, tiles, PAD, 128), BF16),
            pltpu.VMEM((NX, chunks, ny, PAD, feats), BF16),
            pltpu.VMEM((NX, chunks, ny, PAD, feats), BF16),
            pltpu.VMEM((2, n_ep, PAD, feats), BF16),
            pltpu.VMEM((experts, PAD, feats), BF16),
            pltpu.VMEM((toks, 128), F32),
            pltpu.VMEM((2 * toks, experts * PAD), BF16),
            pltpu.VMEM((3, *w_gate.shape), BF16),
            pltpu.VMEM((chunks - chunks // 2, ny - 1, 2 * tiles, PAD, 128), BF16),
            pltpu.VMEM((chunks - chunks // 2, ny - 1, 2 * tiles, PAD, 128), BF16),
            dma, each, dma, dma, dma, dma((3,)), dma, dma, dma, each,
            dma, each, dma, each, dma, each, dma, each, dma, dma((4,)), dma, dma((chunks - chunks // 2, ny - 1)),
        ],
        compiler_params=pltpu.CompilerParams(collective_id=0, has_side_effects=True),
        name="routed_layer",
    )(tokens, norm_gain.reshape(1, feats), route_ids.T, route_gates.T, w_gate, w_up, w_down)
    return mixed


def solution(mesh):
    placed = (
        P("ep", "tp"),
        P("tp"),
        P("ep", None),
        P("ep", None),
        P("ep", None, "tp"),
        P("ep", None, "tp"),
        P("ep", None, "tp"),
    )
    body = functools.partial(layer, mesh.shape["ep"], mesh.shape["tp"])
    return jax.shard_map(body, mesh=mesh, in_specs=placed, out_specs=P("ep", "tp"), check_vma=False)
```

```python
import functools

import jax
import jax.numpy as jnp
from jax import lax
from jax.experimental import pallas as pl
from jax.experimental.pallas import tpu as pltpu
from jax.sharding import PartitionSpec as P

EPSILON = 1e-06
NX = 4
PAD = 16
MESH = pl.DeviceIdType.MESH
F32 = jnp.float32
BF16 = jnp.bfloat16


def dot_nt(a, b):
    return lax.dot_general(a, b, (((1,), (1,)), ((), ())), preferred_element_type=F32)


def dot_nn(a, b):
    return lax.dot_general(a, b, (((1,), (0,)), ((), ())), preferred_element_type=F32)


def kernel(
    n_ep, ny, cap,
    tok_hbm, gain_hbm, ids_hbm, gates_hbm, wg_ref, wu_ref, wd_ref,
    out_ref,
    tok, gain, ids_v, gates,
    zsend, zrecv, xg, wland, wcat, wdn, gain_all, xs, part, direct, ssq, ssq_all,
    hid, po, xr, back, ret, tcol, picks, staged, chain, run,
    z_ss, z_rs, r_ss, r_rs, w_ss, w_rs, g_ss, g_rs, x_ss, x_rs,
    d_ss, d_rs, q_ss, q_rs, h_ss, h_rs, o_ss, o_rs, l_sem, i_sem, y_ss, y_rs,
):
    nz = n_ep // 2
    chunks = n_ep // ny
    rows = ny * PAD
    toks, feats = tok.shape
    experts = 2 * n_ep
    half = wg_ref.shape[1] // 2
    tiles = half // 128
    ep = lax.axis_index("ep")
    tp = lax.axis_index("tp")
    z, core = ep // 2, lax.rem(ep, 2)
    y, x = tp // NX, lax.rem(tp, NX)
    filled = pl.ds(0, cap)

    def z_peer(i):
        j, c = i // 2, lax.rem(i, 2)
        dz = nz // 2 + (1 - 2 * lax.rem(j, 2)) * ((j + 1) // 2)
        return 2 * lax.rem(z + dz, nz) + c

    side = nz // 2

    def slot_of(s):
        lo = lax.rem(s // 2, side)
        return 2 * (4 * (lo // 2) + 2 * (s // 2 // side) + lax.rem(lo, 2)) + lax.rem(s, 2)

    def source_of(n):
        v = n // 2
        return 2 * (side * lax.rem(v // 2, 2) + 2 * (v // 4) + lax.rem(v, 2)) + lax.rem(n, 2)

    mine = slot_of(ep)

    def x_peer(k):
        return lax.rem(x + k, NX)

    def y_peer(k):
        return lax.rem(y + k, ny)

    def on_x(k):
        return dict(device_id=(ep, y * NX + x_peer(k)), device_id_type=MESH)

    def on_y(k):
        return dict(device_id=(ep, y_peer(k) * NX + x), device_id_type=MESH)

    def on_z(to):
        return dict(device_id=(to, tp), device_id_type=MESH)

    def settle(ref, sem):
        pltpu.make_async_copy(ref, ref, sem).wait()

    partner = z * 2 + (1 - core)
    x_steps = (2, 1, 3)
    y_steps = sorted(range(1, ny), key=lambda k: -min(k, ny - k))
    far = 2 * (nz - 1)

    loads = [
        pltpu.make_async_copy(a, b, i_sem.at[n])
        for n, (a, b) in enumerate(((ids_hbm, ids_v), (tok_hbm, tok), (gain_hbm, gain), (gates_hbm, gates)))
    ]
    for load in loads[:2]:
        load.start()

    barrier = pltpu.get_barrier_semaphore()

    def greet(i, carry):
        pl.semaphore_signal(barrier, inc=1, **on_z(z_peer(i)))
        return carry

    lax.fori_loop(0, far, greet, 0)
    pl.semaphore_signal(barrier, inc=1, **on_z(partner))
    for k in x_steps:
        pl.semaphore_signal(barrier, inc=1, **on_x(k))
    for k in y_steps:
        pl.semaphore_signal(barrier, inc=1, **on_y(k))

    for load in loads[2:]:
        load.start()

    def w_src(n, to):
        return staged.at[n, to // 2, pl.ds(pl.multiple_of(lax.rem(to, 2) * half, half), half)]

    weights = (wg_ref, wu_ref, wd_ref)
    for n, ref in enumerate(weights):
        pltpu.make_async_copy(ref, staged.at[n], l_sem).start()
    ret[...] = jnp.zeros_like(ret)
    for load in loads:
        load.wait()

    ids = ids_v[...].astype(F32)
    e_iota = lax.broadcasted_iota(jnp.int32, (experts, toks), 0).astype(F32)
    m0, m1 = e_iota == ids[0:1, :], e_iota == ids[1:2, :]
    named = jnp.where(m0 | m1, 1.0, 0.0).astype(BF16)
    t_row = lax.broadcasted_iota(jnp.int32, (toks, toks), 0)
    t_col = lax.broadcasted_iota(jnp.int32, (toks, toks), 1)
    earlier = jnp.where(t_row < t_col, 1.0, 0.0).astype(BF16)
    before = dot_nn(named, earlier)
    target0 = ids[0:1, :] * PAD + jnp.sum(jnp.where(m0, before, 0.0), axis=0, keepdims=True)
    target1 = ids[1:2, :] * PAD + jnp.sum(jnp.where(m1, before, 0.0), axis=0, keepdims=True)
    size = min(256, experts * PAD)
    for n in range(experts * PAD // size):
        p_iota = (lax.broadcasted_iota(jnp.int32, (size, toks), 0) + n * size).astype(F32)
        pick = jnp.where((p_iota == target0) | (p_iota == target1), 1.0, 0.0).astype(BF16)
        block = dot_nn(pick, tok[...]).astype(BF16)
        zsend[pl.ds(n * size // PAD, size // PAD)] = block.reshape(size // PAD, PAD, feats)
    gain_all[x] = gain[...]
    pl.semaphore_wait(barrier, 2 * nz - 1 + (NX - 1) + (ny - 1))
    settle(staged, l_sem)

    def z_copy(peer):
        return pltpu.make_async_remote_copy(
            src_ref=zsend.at[pl.ds(2 * peer, 2), filled], dst_ref=zrecv.at[:, mine, filled],
            send_sem=z_ss, recv_sem=z_rs.at[mine // ny], **on_z(peer),
        )

    def z_start(i, carry):
        z_copy(z_peer(i)).start()
        return carry


    def send_weight(n):
        for k in x_steps:
            pltpu.make_async_remote_copy(
                src_ref=w_src(n, x_peer(k)), dst_ref=wland.at[n, x],
                send_sem=w_ss, recv_sem=w_rs.at[n], **on_x(k),
            ).start()

    for k in x_steps:
        pltpu.make_async_remote_copy(
            src_ref=gain, dst_ref=gain_all.at[x], send_sem=g_ss, recv_sem=g_rs, **on_x(k)
        ).start()
    send_weight(0)
    send_weight(1)
    lax.fori_loop(0, far, z_start, 0)
    z_copy(partner).start()
    for e in range(2):
        zrecv[e, mine] = zsend[2 * ep + e]
    for n in range(3):
        wland[n, x] = w_src(n, x)[...]

    pad_rows = jnp.zeros((124, toks), F32)
    tcol[...] = jnp.concatenate([target0, target1, gates[...], pad_rows], axis=0).T

    def arrive(c):
        @pl.when(mine // ny == c)
        def _():
            settle(zrecv.at[:, pl.ds(0, ny - 1), filled], z_rs.at[c])

        @pl.when(mine // ny != c)
        def _():
            settle(zrecv.at[:, pl.ds(0, ny), filled], z_rs.at[c])

        for k in x_steps:
            pltpu.make_async_remote_copy(
                src_ref=zrecv.at[x_peer(k) // 2, pl.ds(c * ny, ny), filled],
                dst_ref=xg.at[x, pl.ds(c * ny, ny), filled],
                send_sem=x_ss, recv_sem=x_rs.at[c], **on_x(k),
            ).start()
        xg[x, c * ny : (c + 1) * ny] = zrecv[x // 2, c * ny : (c + 1) * ny]

    longest = ny // 2
    straight = chunks // 2

    def length(c, way):
        return longest if (c + way) % 2 == 0 else ny - 1 - longest

    def place(c, way, s):
        return s - 1 + (length(c, 0) if way else 0)

    def towards(c, way, s):
        left = length(c, way) - s + 1
        return y_peer(left if way == 0 else ny - left)

    def chain_start(c, way, s):
        n, at = c - straight, place(c, way, s)
        src = part.at[c, towards(c, way, s)] if s == 1 else run.at[n, at]
        pltpu.make_async_remote_copy(
            src_ref=src.at[:, filled], dst_ref=chain.at[n, at, :, filled],
            send_sem=y_ss, recv_sem=y_rs.at[n, at], **on_y(1 if way == 0 else ny - 1),
        ).start()

    def chain_end(c, way, s):
        n, at = c - straight, place(c, way, s)
        settle(chain.at[n, at, :, filled], y_rs.at[n, at])
        return chain.at[n, at]

    def hop(s):
        for c in range(straight, chunks):
            for way in range(2):
                if length(c, way) >= s:
                    came = chain_end(c, way, s - 1)[...].astype(F32)
                    run[c - straight, place(c, way, s)] = (came + part[c, towards(c, way, s)].astype(F32)).astype(BF16)
                    chain_start(c, way, s)

    lane = lax.broadcasted_iota(jnp.int32, (rows, 128), 1)
    row = lax.broadcasted_iota(jnp.int32, (rows, 128), 0)

    def gate_up(c):
        settle(xg.at[pl.ds(0, NX - 1), pl.ds(0, ny), filled], x_rs.at[c])
        squares = jnp.zeros((rows, feats), F32)
        for s in range(NX):
            raw = xg[s, c * ny : (c + 1) * ny].reshape(rows, feats).astype(F32)
            squares += raw * raw
            xs[:, s * feats : (s + 1) * feats] = (raw * gain_all[s]).astype(BF16)
        both = dot_nt(xs[...], wcat[...]).astype(BF16)
        for t in range(2 * tiles):
            part[c, :, t] = both[:, t * 128 : (t + 1) * 128].reshape(ny, PAD, 128)
        sums = jnp.sum(squares, axis=1, keepdims=True)
        ssq[c] = jnp.sum(jnp.where(lane == row, sums, 0.0), axis=0, keepdims=True)

    def send_stats(c):
        for k in y_steps:
            pltpu.make_async_remote_copy(
                src_ref=ssq.at[c], dst_ref=ssq_all.at[c, k - 1], send_sem=q_ss, recv_sem=q_rs.at[c], **on_y(k)
            ).start()

    def send_sums(c):
        for k in y_steps:
            pltpu.make_async_remote_copy(
                src_ref=part.at[c, y_peer(k), :, filled], dst_ref=direct.at[c, k - 1, :, filled],
                send_sem=d_ss, recv_sem=d_rs.at[c], **on_y(k),
            ).start()
        send_stats(c)

    def send_chain(c):
        for way in range(2):
            if length(c, way):
                chain_start(c, way, 1)
        send_stats(c)

    def activate(c, chained=False):
        settle(ssq_all.at[c, pl.ds(0, ny - 1)], q_rs.at[c])
        stats = ssq[c] + jnp.sum(ssq_all[c], axis=0)
        held = jnp.where(row[:PAD] + y * PAD == lane[:PAD], stats, 0.0)
        mean = jnp.sum(held, axis=1, keepdims=True) / (feats * NX * ny)
        inverse = lax.rsqrt(mean + EPSILON)
        if chained:
            terms = [chain_end(c, way, length(c, way)) for way in range(2) if length(c, way)]
        else:
            settle(direct.at[c, pl.ds(0, ny - 1), :, filled], d_rs.at[c])
            terms = [direct.at[c, k] for k in range(ny - 1)]

        def summed(t):
            total = part[c, y, t].astype(F32)
            for term in terms:
                total += term[t].astype(F32)
            return total * inverse

        for t in range(tiles):
            gate_act, up_act = summed(t), summed(tiles + t)
            hid[c, y, t] = (gate_act / (1.0 + jnp.exp(-gate_act)) * up_act).astype(BF16)
        for k in y_steps:
            pltpu.make_async_remote_copy(
                src_ref=hid.at[c, y, :, filled], dst_ref=hid.at[c, y, :, filled],
                send_sem=h_ss, recv_sem=h_rs.at[c], **on_y(k),
            ).start()

    def down(c):
        settle(hid.at[c, pl.ds(0, ny - 1), :, filled], h_rs.at[c])
        held = jnp.concatenate([hid[c, :, t].reshape(rows, 128) for t in range(tiles)], axis=1)
        piece = dot_nn(held, wdn[...]).astype(BF16)
        for s in range(NX):
            po[s, c] = piece[:, s * feats : (s + 1) * feats].reshape(ny, PAD, feats)
        for k in x_steps:
            pltpu.make_async_remote_copy(
                src_ref=po.at[x_peer(k), c, :, filled], dst_ref=xr.at[x, c, :, filled],
                send_sem=o_ss, recv_sem=o_rs.at[c], **on_x(k),
            ).start()
        xr[x, c] = po[x, c]

    def r_copy(n):
        return pltpu.make_async_remote_copy(
            src_ref=back.at[:, n, filled], dst_ref=ret.at[pl.ds(2 * ep, 2), filled],
            send_sem=r_ss, recv_sem=r_rs, **on_z(source_of(n)),
        )

    def give_back(c):
        settle(xr.at[pl.ds(0, NX - 1), 0, :, filled], o_rs.at[c])
        for e in range(2):
            back[e, c * ny : (c + 1) * ny] = (xr[2 * e, c].astype(F32) + xr[2 * e + 1, c].astype(F32)).astype(BF16)

        def r_start(i, carry):
            @pl.when(c * ny + i != mine)
            def _():
                r_copy(c * ny + i).start()

            return carry

        lax.fori_loop(0, ny, r_start, 0)

    def join_gate_up():
        settle(gain_all.at[pl.ds(0, NX - 1)], g_rs)
        for n in range(2):
            settle(wland.at[n, pl.ds(0, NX - 1)], w_rs.at[n])
            for s in range(NX):
                wcat[n * half : (n + 1) * half, s * feats : (s + 1) * feats] = wland[n, s]

    def join_down():
        settle(wland.at[2, pl.ds(0, NX - 1)], w_rs.at[2])
        for s in range(NX):
            wdn[:, s * feats : (s + 1) * feats] = wland[2, s]

    p_iota = lax.broadcasted_iota(jnp.int32, (toks, experts * PAD), 1).astype(F32)
    for k in range(2):
        picks[k * toks : (k + 1) * toks] = jnp.where(p_iota == tcol[:, k : k + 1], 1.0, 0.0).astype(BF16)
    for c in range(min(3, chunks)):
        arrive(c)
    join_gate_up()
    for c in range(chunks):
        gate_up(c)
        if c < straight:
            send_sums(c)
        else:

            @pl.when(core == 1)
            def _():
                send_chain(c)

        if c + 3 < chunks:
            arrive(c + 3)
        if c == straight - 1:
            send_weight(2)

    @pl.when(core == 0)
    def _():
        for c in range(straight):
            send_sums(c + straight)
            activate(c)
        join_down()
        down(0)
        for c in range(chunks):
            if c + straight < chunks:
                activate(c + straight)
            if c + 1 < chunks:
                down(c + 1)
            give_back(c)
        settle(direct.at[:, :, :, filled], d_ss)

    @pl.when(core == 1)
    def _():
        for c in range(straight):
            activate(c)
            if c + 2 <= longest:
                hop(c + 2)
        join_down()
        down(0)
        for s in range(straight + 2, longest + 1):
            hop(s)
        for c in range(1, straight):
            down(c)
        give_back(0)
        for c in range(straight, chunks):
            activate(c, True)
        for c in range(1, straight):
            give_back(c)
        for c in range(straight, chunks):
            down(c)
        for c in range(straight, chunks):
            give_back(c)
        settle(direct.at[pl.ds(0, straight), :, :, filled], d_ss)
        settle(chain.at[:, :, :, filled], y_ss)

    for e in range(2):
        ret[2 * ep + e, 0:cap] = back[e, mine, 0:cap]

    settle(zsend.at[pl.ds(0, 2 * (n_ep - 1)), filled], z_ss)
    settle(gain_all.at[pl.ds(0, NX - 1)], g_ss)
    settle(wland.at[:, pl.ds(0, NX - 1)], w_ss)
    settle(xg.at[pl.ds(0, NX - 1), :, filled], x_ss)
    settle(ssq_all, q_ss)
    settle(hid.at[:, pl.ds(0, ny - 1), :, filled], h_ss)
    settle(xr.at[pl.ds(0, NX - 1), :, :, filled], o_ss)

    everyone = ret.at[pl.ds(0, 2 * (n_ep - 1)), filled]
    settle(everyone, r_rs)
    answers = ret[...].reshape(experts * PAD, feats)
    picked = dot_nn(picks[...], answers)
    out_ref[...] = (picked[:toks] * tcol[:, 2:3] + picked[toks:] * tcol[:, 3:4]).astype(BF16)
    settle(everyone, r_ss)


def layer(n_ep, n_tp, tokens, norm_gain, route_ids, route_gates, w_gate, w_up, w_down):
    toks, feats = tokens.shape
    ny = n_tp // NX
    chunks = n_ep // ny
    experts = 2 * n_ep
    cap = max(2, (5 * toks * 2 + 4 * experts - 1) // (4 * experts))
    half = w_gate.shape[1] // 2
    tiles = half // 128
    dma = pltpu.SemaphoreType.DMA
    each = pltpu.SemaphoreType.DMA((chunks,))
    hbm = pl.BlockSpec(memory_space=pl.ANY)
    mixed = pl.pallas_call(
        functools.partial(kernel, n_ep, ny, cap),
        out_shape=pltpu.VMEM((toks, feats), BF16),
        in_specs=[hbm] * 7,
        out_specs=pl.BlockSpec(memory_space=pltpu.VMEM),
        scratch_shapes=[
            pltpu.VMEM((toks, feats), BF16),
            pltpu.VMEM((1, feats), F32),
            pltpu.VMEM((2, toks), jnp.int32),
            pltpu.VMEM((2, toks), F32),
            pltpu.VMEM((experts, PAD, feats), BF16),
            pltpu.VMEM((2, n_ep, PAD, feats), BF16),
            pltpu.VMEM((NX, n_ep, PAD, feats), BF16),
            pltpu.VMEM((3, NX, half, feats), BF16),
            pltpu.VMEM((2 * half, NX * feats), BF16),
            pltpu.VMEM((half, NX * feats), BF16),
            pltpu.VMEM((NX, 1, feats), F32),
            pltpu.VMEM((ny * PAD, NX * feats), BF16),
            pltpu.VMEM((chunks, ny, 2 * tiles, PAD, 128), BF16),
            pltpu.VMEM((chunks, ny - 1, 2 * tiles, PAD, 128), BF16),
            pltpu.VMEM((chunks, 1, 128), F32),
            pltpu.VMEM((chunks, ny - 1, 1, 128), F32),
            pltpu.VMEM((chunks, ny, tiles, PAD, 128), BF16),
            pltpu.VMEM((NX, chunks, ny, PAD, feats), BF16),
            pltpu.VMEM((NX, chunks, ny, PAD, feats), BF16),
            pltpu.VMEM((2, n_ep, PAD, feats), BF16),
            pltpu.VMEM((experts, PAD, feats), BF16),
            pltpu.VMEM((toks, 128), F32),
            pltpu.VMEM((2 * toks, experts * PAD), BF16),
            pltpu.VMEM((3, *w_gate.shape), BF16),
            pltpu.VMEM((chunks - chunks // 2, ny - 1, 2 * tiles, PAD, 128), BF16),
            pltpu.VMEM((chunks - chunks // 2, ny - 1, 2 * tiles, PAD, 128), BF16),
            dma, each, dma, dma, dma, dma((3,)), dma, dma, dma, each,
            dma, each, dma, each, dma, each, dma, each, dma, dma((4,)), dma, dma((chunks - chunks // 2, ny - 1)),
        ],
        compiler_params=pltpu.CompilerParams(collective_id=0, has_side_effects=True),
        name="routed_layer",
    )(tokens, norm_gain.reshape(1, feats), route_ids.T, route_gates.T, w_gate, w_up, w_down)
    return mixed


def solution(mesh):
    placed = (
        P("ep", "tp"),
        P("tp"),
        P("ep", None),
        P("ep", None),
        P("ep", None, "tp"),
        P("ep", None, "tp"),
        P("ep", None, "tp"),
    )
    body = functools.partial(layer, mesh.shape["ep"], mesh.shape["tp"])
    return jax.shard_map(body, mesh=mesh, in_specs=placed, out_specs=P("ep", "tp"), check_vma=False)
```
